32 devices in a mesh: sp: 8 (over z, y), tp: 4 (over x, core).
Axes of the slice: x: 2, y: 2, z: 4, core: 2. Of those that a mesh axis runs over, the one named last changes fastest.
Arguments:
- residual: bfloat16 [8192, 2048], P('sp'), may hold values from -6 to 6
- small_heads: bfloat16 [8192, 1024], P('sp', 'tp'), may hold values from -6 to 6
- large_heads: bfloat16 [8192, 1024], P('sp', 'tp'), may hold values from -6 to 6
- state_keys: bfloat16 [8192, 8, 128], P('sp', 'tp'), may hold values from -6 to 6
- state_queries: bfloat16 [8192, 8, 128], P('sp', 'tp'), may hold values from -6 to 6
- small_gate: bfloat16 [8192, 1024], P('sp', 'tp'), may hold values from -6 to 6
- large_gate: bfloat16 [8192, 1024], P('sp', 'tp'), may hold values from -6 to 6
- small_step: float32 [8192, 16], P('sp', 'tp'), may hold values from -3 to 2
- large_step: float32 [8192, 8], P('sp', 'tp'), may hold values from -3 to 2
- small_taps: bfloat16 [4, 1024], P(None, 'tp'), may hold values from -3 to 3
- large_taps: bfloat16 [4, 1024], P(None, 'tp'), may hold values from -3 to 3
- key_taps: bfloat16 [4, 8, 128], P(None, 'tp'), may hold values from -3 to 3
- query_taps: bfloat16 [4, 8, 128], P(None, 'tp'), may hold values from -3 to 3
- small_decay: float32 [16], P('tp'), may hold values from -12 to -2, as said below
- large_decay: float32 [8], P('tp'), may hold values from -12 to -2, as said below
- small_gain: bfloat16 [1024], P('tp'), may hold values from 0.099609375 to 1.8984375
- large_gain: bfloat16 [1024], P('tp'), may hold values from 0.099609375 to 1.8984375
- small_out: bfloat16 [1024, 2048], P('tp'), may hold values from -0.125 to 0.125
- large_out: bfloat16 [1024, 2048], P('tp'), may hold values from -0.125 to 0.125
- mixer_gain: bfloat16 [2048], replicated, may hold values from 0.099609375 to 1.8984375
- ffn_in_gain: bfloat16 [2048], replicated, may hold values from 0.099609375 to 1.8984375
- gate_proj: bfloat16 [2048, 5632], P('sp', 'tp'), may hold values from -0.125 to 0.125
- up_proj: bfloat16 [2048, 5632], P('sp', 'tp'), may hold values from -0.125 to 0.125
- down_proj: bfloat16 [2048, 5632], P('sp', 'tp'), may hold values from -0.078125 to 0.078125
- ffn_out_gain: bfloat16 [2048], replicated, may hold values from 0.099609375 to 1.8984375
Outputs:
- updated: bfloat16 [8192, 2048], P(('sp', 'tp'))
The draws below stay inside these ranges and needn't reach their ends.
Inputs may be any that keep to these rules, and one draw needn't show every extreme that they name: `small_decay`: log decay rates of the first group. `large_decay`: log decay rates of the second group.
All inputs are finite; a program needn't handle non-finite values.
Results may differ from the reference program's by a relative error of at most 0.014.
Values may be sent and summed in bfloat16 or wider, within the bound.
A program may use at most 192 MiB of HBM per device.

```python
import jax
import jax.numpy as jnp
from jax import lax

D = 2048
FF = 5632
HA = 16
PA = 64
HB = 8
PB = 128
GROUPS = 8
STATE = 128
CONV = 4
BLOCK = 128
TOK_DEV = 1024
TOKENS = 8192
HEAD_BLOCKS = 4


def step_law(key, heads, salt):
    rows = jnp.arange(TOKENS, dtype=jnp.int32) // TOK_DEV
    offset_key = jax.random.fold_in(key, 101)
    jitter_key = jax.random.fold_in(key, salt)
    offsets = jax.random.uniform(offset_key, (TOKENS // TOK_DEV,), jnp.float32, -1.5, 0.5)
    jitter = jnp.clip(0.5 * jax.random.normal(jitter_key, (TOKENS, heads), jnp.float32), -1.5, 1.5)
    return offsets[rows][:, None] + jitter


def decay_law(key, heads, salt):
    base_key = jax.random.fold_in(key, salt)
    order_key, slow_key, fast_key = jax.random.split(base_key, 3)
    fast_count = heads // 2
    ranks = jax.random.permutation(order_key, heads)
    slow_values = jnp.log(jax.random.uniform(slow_key, (heads,), jnp.float32, 0.25, 1.5) / TOKENS)
    fast_values = jnp.log(jax.random.uniform(fast_key, (heads,), jnp.float32, 1.0 / 60.0, 1.0 / 20.0))
    return jnp.where(ranks < fast_count, fast_values, slow_values)


def draw_small_step(key, part):
    return step_law(key, HA, 11)


def draw_large_step(key, part):
    return step_law(key, HB, 12)


def draw_small_decay(key, part):
    return decay_law(key, HA, 21)


def draw_large_decay(key, part):
    return decay_law(key, HB, 22)


def shard_levels(rng, shape, pieces, low, top_value):
    def one(position, parts):
        draws = jax.random.uniform(jax.random.fold_in(jax.random.fold_in(rng, 6), position), (parts,), jnp.float32, low / len(pieces), top_value / len(pieces))
        return jnp.repeat(jnp.exp(draws), shape[position] // parts).reshape((-1,) + (1,) * (len(shape) - position - 1))

    loudness = one(*pieces[0])
    for cut in pieces[1:]:
        loudness = loudness * one(*cut)
    return loudness


def scatter_about(rng, shape, width, bound, cuts=(), kind=jnp.bfloat16):
    level = shard_levels(rng, shape, cuts, -0.22, 0.18) if cuts else 1.0
    drawn = jax.random.normal(rng, shape, jnp.float32) * width * level
    return jnp.minimum(jnp.maximum(drawn, -bound), bound).astype(kind)


def setup_inputs(seed: int = 0) -> dict:
    arg_keys = jax.random.split(jax.random.key(seed), 26)
    return {
        "residual": scatter_about(arg_keys[0], (TOKENS, D), 1.0, 6.0, ((0, 8),)),
        "small_heads": scatter_about(arg_keys[1], (TOKENS, HA * PA), 1.0, 6.0, ((0, 8), (1, 4))),
        "large_heads": scatter_about(arg_keys[2], (TOKENS, HB * PB), 1.0, 6.0, ((0, 8), (1, 4))),
        "state_keys": scatter_about(arg_keys[3], (TOKENS, GROUPS, STATE), 1.0, 6.0, ((0, 8), (1, 4))),
        "state_queries": scatter_about(arg_keys[4], (TOKENS, GROUPS, STATE), 1.0, 6.0, ((0, 8), (1, 4))),
        "small_gate": scatter_about(arg_keys[5], (TOKENS, HA * PA), 1.0, 6.0, ((0, 8), (1, 4))),
        "large_gate": scatter_about(arg_keys[6], (TOKENS, HB * PB), 1.0, 6.0, ((0, 8), (1, 4))),
        "small_step": draw_small_step(jax.random.fold_in(arg_keys[25], 71), 0),
        "large_step": draw_large_step(jax.random.fold_in(arg_keys[25], 71), 0),
        "small_taps": scatter_about(arg_keys[9], (CONV, HA * PA), CONV ** -0.5, 3.0, ((1, 4),)),
        "large_taps": scatter_about(arg_keys[10], (CONV, HB * PB), CONV ** -0.5, 3.0, ((1, 4),)),
        "key_taps": scatter_about(arg_keys[11], (CONV, GROUPS, STATE), CONV ** -0.5, 3.0, ((1, 4),)),
        "query_taps": scatter_about(arg_keys[12], (CONV, GROUPS, STATE), CONV ** -0.5, 3.0, ((1, 4),)),
        "small_decay": draw_small_decay(jax.random.fold_in(arg_keys[25], 71), 0),
        "large_decay": draw_large_decay(jax.random.fold_in(arg_keys[25], 71), 0),
        "small_gain": jnp.clip(1.0 + 0.18 * jax.random.normal(arg_keys[15], (HA * PA,), jnp.float32), 0.099609375, 1.8984375).astype(jnp.bfloat16),
        "large_gain": jnp.clip(1.0 + 0.18 * jax.random.normal(arg_keys[16], (HB * PB,), jnp.float32), 0.099609375, 1.8984375).astype(jnp.bfloat16),
        "small_out": scatter_about(arg_keys[17], (HA * PA, D), (HA * PA + HB * PB) ** -0.5, 0.125, ((0, 4),)),
        "large_out": scatter_about(arg_keys[18], (HB * PB, D), (HA * PA + HB * PB) ** -0.5, 0.125, ((0, 4),)),
        "mixer_gain": jnp.clip(1.0 + 0.18 * jax.random.normal(arg_keys[19], (D,), jnp.float32), 0.099609375, 1.8984375).astype(jnp.bfloat16),
        "ffn_in_gain": jnp.clip(1.0 + 0.18 * jax.random.normal(arg_keys[20], (D,), jnp.float32), 0.099609375, 1.8984375).astype(jnp.bfloat16),
        "gate_proj": scatter_about(arg_keys[21], (D, FF), D ** -0.5, 0.125, ((0, 8), (1, 4))),
        "up_proj": scatter_about(arg_keys[22], (D, FF), D ** -0.5, 0.125, ((0, 8), (1, 4))),
        "down_proj": scatter_about(arg_keys[23], (D, FF), FF ** -0.5, 0.078125, ((0, 8), (1, 4))),
        "ffn_out_gain": jnp.clip(1.0 + 0.18 * jax.random.normal(arg_keys[24], (D,), jnp.float32), 0.099609375, 1.8984375).astype(jnp.bfloat16),
    }


EPS = 1e-06

def rounded(values):
    return lax.optimization_barrier(values.astype(jnp.bfloat16)).astype(jnp.float32)

def causal_taps(extended, tap_weights, length):
    kernel_len = tap_weights.shape[0]
    summed = jnp.zeros((length,) + extended.shape[1:], jnp.float32)
    for offset in range(kernel_len):
        window_rows = extended[offset:offset + length].astype(jnp.float32)
        summed = summed + tap_weights[offset].astype(jnp.float32) * window_rows
    return jax.nn.silu(summed).astype(jnp.bfloat16)

def block_pass(values, key_rows, queries, step_sizes, decay_rates):
    length, groups, head_count, head_dim = values.shape
    block_count = length // BLOCK
    state_len = key_rows.shape[-1]
    log_decay = -step_sizes * decay_rates
    causal = jnp.tril(jnp.ones((BLOCK, BLOCK), dtype=bool))
    highest = lax.Precision.HIGHEST

    def one_block(carry_state, block):
        block_values, block_keys, block_queries, block_steps, block_decay = block
        values_wide = block_values.astype(jnp.float32)
        keys_wide = block_keys.astype(jnp.float32)
        queries_wide = block_queries.astype(jnp.float32)
        cumulative = jnp.cumsum(block_decay, axis=0)
        scores = jnp.einsum('lgn,sgn->gls', queries_wide, keys_wide, precision=highest)
        cum_heads = jnp.transpose(cumulative, (1, 2, 0))
        gap_matrix = cum_heads[:, :, :, None] - cum_heads[:, :, None, :]
        decays = jnp.exp(jnp.where(causal, gap_matrix, -jnp.inf))
        step_heads = jnp.transpose(block_steps, (1, 2, 0))[:, :, None, :]
        weights = rounded(scores[:, None] * decays * step_heads)
        inside = jnp.einsum('ghls,sghp->lghp', weights, values_wide, precision=highest)
        carried = jnp.einsum('lgn,ghpn->lghp', queries_wide, carry_state, precision=highest)
        carried = carried * jnp.exp(cumulative)[..., None]
        tail_sum = cumulative[-1]
        scaled = rounded(values_wide * (block_steps * jnp.exp(tail_sum - cumulative))[..., None])
        fresh_state = jnp.einsum('lghp,lgn->ghpn', scaled, keys_wide, precision=highest)
        next_state = carry_state * jnp.exp(tail_sum)[..., None, None] + fresh_state
        return (next_state, inside + carried)
    blocked = (values.reshape(block_count, BLOCK, groups, head_count, head_dim), key_rows.reshape(block_count, BLOCK, groups, state_len), queries.reshape(block_count, BLOCK, groups, state_len), step_sizes.reshape(block_count, BLOCK, groups, head_count), log_decay.reshape(block_count, BLOCK, groups, head_count))
    start_state = jnp.zeros((groups, head_count, head_dim, state_len), jnp.float32)
    end_state, outputs = lax.scan(one_block, start_state, blocked)
    return outputs.reshape(length, groups, head_count, head_dim)

def head_group(values, key_rows, queries, step_raw, decay_log):
    length = values.shape[0]
    head_count = step_raw.shape[1]
    groups = key_rows.shape[1]
    per_group = head_count // groups
    head_dim = values.shape[1] // head_count
    step_sizes = jax.nn.softplus(step_raw.astype(jnp.float32)).reshape(length, groups, per_group)
    decay_rates = jnp.exp(decay_log.astype(jnp.float32)).reshape(groups, per_group)
    return block_pass(values.reshape(length, groups, per_group, head_dim), key_rows, queries, step_sizes, decay_rates)

def unit_rms(values):
    return values * lax.rsqrt(lax.optimization_barrier(jnp.mean(values * values, axis=-1, keepdims=True)) + EPS)

def gate_and_norm(mixed_heads, gate_raw, gain):
    length, groups, per_group, head_dim = mixed_heads.shape
    gated = mixed_heads.reshape(length, -1) * jax.nn.silu(gate_raw.astype(jnp.float32))
    normed = unit_rms(gated.reshape(length, groups * per_group, head_dim))
    return (normed.reshape(length, -1) * gain.astype(jnp.float32)).astype(jnp.bfloat16)

def blockwise_sum(pairs, length, features):
    summed = jnp.zeros((length, features), jnp.float32)
    for index in range(HEAD_BLOCKS):
        partial_value = jnp.zeros((length, features), jnp.float32)
        for left, right in pairs:
            cols = left.shape[1] // HEAD_BLOCKS
            partial_value = partial_value + jnp.dot(left[:, index * cols:(index + 1) * cols], right[index * cols:(index + 1) * cols], preferred_element_type=jnp.float32)
        summed = summed + rounded(partial_value)
    return summed

def reference(residual, small_heads, large_heads, state_keys, state_queries, small_gate, large_gate, small_step, large_step, small_taps, large_taps, key_taps, query_taps, small_decay, large_decay, small_gain, large_gain, small_out, large_out, mixer_gain, ffn_in_gain, gate_proj, up_proj, down_proj, ffn_out_gain):
    length = residual.shape[0]
    halo_rows = small_taps.shape[0] - 1

    def extended(values):
        return jnp.concatenate([jnp.zeros((halo_rows,) + values.shape[1:], values.dtype), values], axis=0)
    small_conv = causal_taps(extended(small_heads), small_taps, length)
    large_conv = causal_taps(extended(large_heads), large_taps, length)
    key_conv = causal_taps(extended(state_keys), key_taps, length)
    query_conv = causal_taps(extended(state_queries), query_taps, length)
    small_mix = head_group(small_conv, key_conv[:, 0::2], query_conv[:, 0::2], small_step, small_decay)
    large_mix = head_group(large_conv, key_conv[:, 1::2], query_conv[:, 1::2], large_step, large_decay)
    small_normed = gate_and_norm(small_mix, small_gate, small_gain)
    large_normed = gate_and_norm(large_mix, large_gate, large_gain)
    mix = blockwise_sum([(small_normed, small_out), (large_normed, large_out)], length, D)
    mixed = residual.astype(jnp.float32) + unit_rms(mix) * mixer_gain.astype(jnp.float32)
    normed_in = (unit_rms(mixed) * ffn_in_gain.astype(jnp.float32)).astype(jnp.bfloat16)
    gate = jnp.dot(normed_in, gate_proj, preferred_element_type=jnp.float32)
    up_values = jnp.dot(normed_in, up_proj, preferred_element_type=jnp.float32)
    hidden = (jax.nn.silu(gate) * up_values).astype(jnp.bfloat16)
    ffn = blockwise_sum([(hidden, jnp.transpose(down_proj))], length, D)
    updated = mixed + 0.5 * unit_rms(ffn) * ffn_out_gain.astype(jnp.float32)
    return updated.astype(jnp.bfloat16)
```

```python
import functools

import jax
import jax.numpy as jnp
from jax import lax
from jax.experimental import pallas as pl
from jax.experimental.pallas import tpu as pltpu
from jax.sharding import PartitionSpec as P

BLOCK = 128
HALO = 16
LANES = 128
SLOTS = 8
TAIL = 16


EPS = 1e-06
OUTER, INNER = "so", "si"
SEQ = (OUTER, INNER)
CHIP, CORE = "tx", "tc"
HEADS = (CHIP, CORE)
MESH = pl.DeviceIdType.MESH
VMEM_BYTES = 64 * 1024 * 1024 - 128 * 1024
FAR = -1e30
F32 = jnp.float32
BF16 = jnp.bfloat16


def moved(block, axis, route):
    return lax.ppermute(block, axis, route)


def earlier(block, axis, distance):
    devices = range(lax.axis_size(axis))
    return moved(block, axis, [(i - distance, i) for i in devices if i - distance in devices])


def paired(block, axis, bit):
    return moved(block, axis, [(i, i ^ bit) for i in range(lax.axis_size(axis))])


def silu(x):
    return x / (1.0 + jnp.exp(-x))


def softplus(x):
    return jnp.maximum(x, 0.0) + jnp.log1p(jnp.exp(-jnp.abs(x)))


def exact_dot(a, b):
    return lax.dot_general(
        a, b, (((1,), (0,)), ((), ())), precision=lax.Precision.HIGHEST, preferred_element_type=F32
    )


def lower(n):
    rows = lax.broadcasted_iota(jnp.int32, (n, n), 0)
    return rows >= lax.broadcasted_iota(jnp.int32, (n, n), 1)


def spread(columns, heads, dim):
    rows = columns.shape[0]
    parts = []
    if dim >= LANES:
        for h in heads:
            parts.append(jnp.broadcast_to(columns[:, h : h + 1], (rows, dim)))
    else:
        per = LANES // dim
        lane = lax.broadcasted_iota(jnp.int32, (rows, LANES), 1)
        for first in range(0, len(heads), per):
            part = jnp.broadcast_to(columns[:, heads[first] : heads[first] + 1], (rows, LANES))
            for j in range(1, per):
                h = heads[first + j]
                part = jnp.where(lane >= j * dim, columns[:, h : h + 1], part)
            parts.append(part)
    return jnp.concatenate(parts, axis=1)


def conv_kernel(
    sizes, small, large, keys, queries, halo, taps, steps, decay, conv, packed, before, state, total
):
    (heads_a, dim_a), (heads_b, dim_b), state_len = sizes
    step = pl.program_id(0)

    @pl.when(step == 0)
    def _():
        before[...] = halo[...]
        state[...] = jnp.zeros_like(state)
        total[...] = jnp.zeros_like(total)

    column = 0
    for ref in (small, large, keys, queries):
        width = ref.shape[1]
        for start in range(0, width, LANES):
            here = pl.ds(column, LANES)
            now = ref[:, pl.ds(start, LANES)]
            extended = jnp.concatenate([before[:, here], now], axis=0).astype(F32)
            kernel_len = taps.shape[0]
            summed = None
            for k in range(kernel_len):
                first = HALO - kernel_len + 1 + k
                term = taps[k : k + 1, here] * extended[first : first + BLOCK]
                summed = term if summed is None else summed + term
            done = silu(summed).astype(BF16)
            conv[:, here] = done
            before[:, here] = now[BLOCK - HALO :]
            column += LANES
    dt = softplus(steps[...])
    cum = exact_dot(lower(BLOCK).astype(F32), -dt * jnp.exp(decay[...]))
    tail = cum[BLOCK - 1 : BLOCK]
    scale = dt * jnp.exp(tail - cum)
    head_list_a = list(range(heads_a))
    head_list_b = list(range(heads_a, heads_a + heads_b))
    kept = jnp.exp(tail)
    offset = 0
    width_a = heads_a * dim_a
    width_b = heads_b * dim_b
    for heads, dim, width, key_at in (
        (head_list_a, dim_a, width_a, width_a + width_b),
        (head_list_b, dim_b, width_b, width_a + width_b + state_len),
    ):
        x = conv[:, offset : offset + width].astype(F32)
        u = (x * spread(scale, heads, dim)).astype(BF16)
        k = conv[:, key_at : key_at + state_len]
        fresh = lax.dot_general(k, u, (((0,), (0,)), ((), ())), preferred_element_type=F32)
        old = state[:, offset : offset + width]
        state[:, offset : offset + width] = old * spread(kept, heads, dim) + fresh
        offset += width
    total[...] = total[...] + tail

    @pl.when(step == pl.num_programs(0) - 1)
    def _():
        packed[:state_len] = state[...].astype(BF16)
        whole = jnp.concatenate(
            [spread(total[...], head_list_a, dim_a), spread(total[...], head_list_b, dim_b)], axis=1
        )
        high = whole.astype(BF16)
        low = (whole - high.astype(F32)).astype(BF16)
        row = lax.broadcasted_iota(jnp.int32, (TAIL, whole.shape[1]), 0)
        both = jnp.where(row == 0, high.astype(F32), jnp.where(row == 1, low.astype(F32), 0.0))
        packed[state_len:] = both.astype(BF16)


def mix_kernel(
    sizes,
    place,
    conv,
    small_gate,
    large_gate,
    steps,
    steps_across,
    decay,
    decay_across,
    gain,
    small_out,
    large_out,
    entering,
    partial_out,
    state,
):
    (heads_a, dim_a), (heads_b, dim_b), state_len = sizes
    step = pl.program_id(0)

    @pl.when(step == 0)
    def _():
        state[...] = entering[...]

    causal = lower(BLOCK)
    ones = causal.astype(F32)
    dt = softplus(steps[...])
    cum = exact_dot(ones, -dt * jnp.exp(decay[...]))
    dt_across = softplus(steps_across[...])
    upper = (
        lax.broadcasted_iota(jnp.int32, (BLOCK, BLOCK), 0)
        <= lax.broadcasted_iota(jnp.int32, (BLOCK, BLOCK), 1)
    ).astype(F32)
    cum_across = exact_dot(-dt_across * jnp.exp(decay_across[...]), upper)
    tail = cum[BLOCK - 1 : BLOCK]
    scale = dt * jnp.exp(tail - cum)
    grown = jnp.exp(cum)
    kept = jnp.exp(tail)
    width_a = heads_a * dim_a
    width_b = heads_b * dim_b
    offset = 0
    result = None
    lane = lax.broadcasted_iota(jnp.int32, (BLOCK, LANES), 1)
    for which, (heads, dim, width, gate, out) in enumerate(
        (
            (list(range(heads_a)), dim_a, width_a, small_gate, small_out),
            (list(range(heads_a, heads_a + heads_b)), dim_b, width_b, large_gate, large_out),
        )
    ):
        key_at = width_a + width_b + which * state_len
        query_at = key_at + 2 * state_len
        x = conv[:, offset : offset + width]
        k = conv[:, key_at : key_at + state_len]
        q = conv[:, query_at : query_at + state_len]
        scores = lax.dot_general(q, k, (((1,), (1,)), ((), ())), preferred_element_type=F32)
        old = state[:, offset : offset + width]
        carried = jnp.dot(q, old.astype(BF16), preferred_element_type=F32)
        carried = carried * spread(grown, heads, dim)
        u = (x.astype(F32) * spread(scale, heads, dim)).astype(BF16)
        fresh = lax.dot_general(k, u, (((0,), (0,)), ((), ())), preferred_element_type=F32)
        state[:, offset : offset + width] = old * spread(kept, heads, dim) + fresh
        inside = []
        span = max(dim, LANES)
        per = span // dim
        for first in range(0, len(heads), per):
            x_part = x[:, first * dim : first * dim + span]
            part = None
            for j in range(per):
                h = heads[first + j]
                gap = cum[:, h : h + 1] - cum_across[h : h + 1]
                decays = jnp.exp(jnp.where(causal, gap, FAR))
                w = (scores * decays * dt_across[h : h + 1]).astype(BF16)
                got = jnp.dot(w, x_part, preferred_element_type=F32)
                part = got if part is None else jnp.where(lane >= j * dim, got, part)
            inside.append(part)
        mixed = jnp.concatenate(inside, axis=1) + carried
        gated = mixed * silu(gate[...].astype(F32))
        squares = gated * gated
        normed = []
        for first in range(0, len(heads), per):
            at = first * dim
            part = squares[:, at : at + span]
            means = None
            for j in range(per):
                if per == 1:
                    means = jnp.sum(part, axis=1, keepdims=True)
                else:
                    ours = (lane >= j * dim) & (lane < (j + 1) * dim)
                    one = jnp.sum(jnp.where(ours, part, 0.0), axis=1, keepdims=True)
                    means = one if means is None else jnp.where(lane >= j * dim, one, means)
            normed.append(gated[:, at : at + span] * lax.rsqrt(means * (1.0 / dim) + EPS))
        normed = jnp.concatenate(normed, axis=1) * gain[:, offset : offset + width]
        product = jnp.dot(normed.astype(BF16), out[...], preferred_element_type=F32)
        result = product if result is None else result + product
        offset += width
    partial_out[...] = result.astype(BF16)[None]


def unit_rms(values):
    return values * lax.rsqrt(jnp.mean(values * values, axis=-1, keepdims=True) + EPS)


def norm_kernel(one, other, own, mixer_gain, ffn_gain, mixed_out, normed_out):
    mix = one[...].astype(F32) + other[...].astype(F32)
    mixed = own[...].astype(F32) + unit_rms(mix) * mixer_gain[...].astype(F32)
    mixed_out[...] = mixed
    normed_out[...] = (unit_rms(mixed) * ffn_gain[...].astype(F32)).astype(BF16)


def half_width(columns):
    return (columns // LANES + 1) // 2 * LANES


def greet(partners):
    barrier = pltpu.get_barrier_semaphore()
    for partner in partners:
        pl.semaphore_signal(barrier, inc=1, device_id=partner, device_id_type=MESH)
    pl.semaphore_wait(barrier, len(partners))


def remote(source, target, send, recv, partner):
    copy = pltpu.make_async_remote_copy(
        src_ref=source,
        dst_ref=target,
        send_sem=send,
        recv_sem=recv,
        device_id=partner,
        device_id_type=MESH,
    )
    return copy


def weights_kernel(count, sources, targets, sems):
    send, recv, side_send, side_recv, local_sem = sems
    z, y = lax.axis_index(OUTER), lax.axis_index(INNER)
    rows, columns = sources[0].shape
    wide = targets[0].shape[1]
    partner = {INNER: 1 - y}
    others = {d: (z + d) % count for d in range(1, count)}
    greet([partner] + [{OUTER: other} for other in others.values()])

    def half(ref, member):
        start = pl.multiple_of(member % 2 * (columns - wide), LANES)
        return ref.at[:, pl.ds(start, wide)]

    def block(ref, index):
        return ref.at[pl.ds(pl.multiple_of((index * 2 + y) * rows, rows), rows)]

    order = sorted(others, key=lambda d: (min(d, count - d), d))
    sent, passed, kept = [], [], []
    for m, (source, target) in enumerate(zip(sources, targets)):
        for d in order:
            copy = remote(
                half(source, others[d]), block(target, z), send.at[m, d], recv.at[m, d], {OUTER: others[d]}
            )
            copy.start()
            sent.append(copy)
        copy = remote(half(source, z), block(target, z), side_send.at[m, 0], side_recv.at[m, 0], partner)
        copy.start()
        passed.append(copy)
        copy = pltpu.make_async_copy(half(source, z), block(target, z), local_sem.at[m])
        copy.start()
        kept.append(copy)
    for m, target in enumerate(targets):
        for d in order:
            here = block(target, (z + count - d) % count)
            remote(here, here, send.at[m, d], recv.at[m, d], partner).wait_recv()
            copy = remote(here, here, side_send.at[m, d], side_recv.at[m, d], partner)
            copy.start()
            passed.append(copy)
    for copy in kept:
        copy.wait()
    for copy in sent:
        copy.wait_send()
    for copy in passed:
        copy.wait()


def gather_weights_kernel(count, gate, up, down, gate_out, up_out, down_out, *sems):
    weights_kernel(count, (gate, up, down), (gate_out, up_out, down_out), sems)


def gathered(*shards):
    rows, columns = shards[0].shape
    count = lax.axis_size(OUTER)
    wide = half_width(columns)
    n = len(shards)
    return pl.pallas_call(
        functools.partial(gather_weights_kernel, count),
        in_specs=[pl.BlockSpec(memory_space=pl.ANY)] * n,
        out_specs=[pl.BlockSpec(memory_space=pltpu.VMEM)] * n,
        out_shape=[jax.ShapeDtypeStruct((2 * count * rows, wide), BF16)] * n,
        scratch_shapes=[pltpu.SemaphoreType.DMA((n, count))] * 4 + [pltpu.SemaphoreType.DMA((n,))],
        compiler_params=pltpu.CompilerParams(
            collective_id=0, has_side_effects=True, vmem_limit_bytes=VMEM_BYTES
        ),
        cost_estimate=pl.CostEstimate(flops=1_000_000_000, bytes_accessed=rows, transcendentals=0),
        name="weights",
    )(*shards)


def ffn_kernel(
    overlap,
    normed,
    gate_weights,
    up_weights,
    down_weights,
    mixed,
    gain,
    out,
    blocks,
    local,
    to_core,
    from_core,
    hop,
    got,
    send,
    recv,
    core_send,
    core_recv,
    hop_send,
    hop_recv,
):
    z, x, c = lax.axis_index(OUTER), lax.axis_index(CHIP), lax.axis_index(CORE)
    pair = z % 2

    def flipped(value, by):
        return value + by * (1 - 2 * value)

    def place(core, d_one, d_two):
        dz = d_one * (1 - core) + d_two * core
        dx = d_one * core + d_two * (1 - core)
        return (flipped(pair, dz) * 2 + flipped(x, dx)) * 2 + core

    near = {CORE: 1 - c}
    one = {OUTER: z + (1 - c) * (1 - 2 * pair), CHIP: flipped(x, c)}
    two = {OUTER: z + c * (1 - 2 * pair), CHIP: flipped(x, 1 - c)}
    greet([near, one, two])
    mine = place(c, 0, 0)
    starts = []
    for index, partner in enumerate((one, two, near)):
        copy = remote(normed, blocks.at[mine], send.at[index], recv.at[mine], partner)
        copy.start()
        starts.append(copy)
    blocks[mine] = normed[...]

    def passing(slot, index, partner):
        return remote(blocks.at[slot], blocks.at[slot], send.at[index], recv.at[slot], partner)

    def product(slot):
        rows = blocks[slot]
        gate = jnp.dot(rows, gate_weights[...], preferred_element_type=F32)
        up = jnp.dot(rows, up_weights[...], preferred_element_type=F32)
        hidden = silu(gate) * up
        column = lax.broadcasted_iota(jnp.int32, hidden.shape, 1)
        hidden = jnp.where(column >= pair * overlap, hidden, 0.0).astype(BF16)
        return lax.dot_general(
            hidden, down_weights[...], (((1,), (1,)), ((), ())), preferred_element_type=F32
        )

    def to_near(j):
        return remote(to_core.at[j], from_core.at[j], core_send.at[j], core_recv.at[j], near)

    def step(j, _):
        d_one, d_two = j % 2, j // 2
        slot = place(c, d_one, d_two)

        @pl.when(j > 0)
        def _():
            passing(slot, 0, near).wait_recv()
            passing(slot, 3 + j, near).start()

        @pl.when(j == 1)
        def _():
            passing(slot, 3, two).start()

        local[j] = product(slot)
        slot = place(1 - c, d_one, d_two)
        passing(slot, 0, near).wait_recv()
        to_core[j] = product(slot).astype(BF16)
        to_near(j).start()
        return 0

    lax.fori_loop(0, 4, step, 0)

    def hopping(index, partner):
        return remote(hop.at[index], got.at[index], hop_send.at[index], hop_recv.at[index], partner)

    def chip_sum(j):
        to_near(j).wait_recv()
        return local[j] + from_core[j].astype(F32)

    hop[0] = chip_sum(3).astype(BF16)
    hopping(0, two).start()
    hop[1] = chip_sum(2).astype(BF16)
    hopping(1, two).start()
    partial = chip_sum(1)
    hopping(0, two).wait_recv()
    hop[2] = (partial + got[0].astype(F32)).astype(BF16)
    hopping(2, one).start()
    total = chip_sum(0)
    hopping(1, two).wait_recv()
    total = total + got[1].astype(F32)
    hopping(2, one).wait_recv()
    total = total + got[2].astype(F32)
    out[...] = (mixed[...] + 0.5 * unit_rms(total) * gain[...].astype(F32)).astype(BF16)
    for copy in starts:
        copy.wait_send()
    passing(mine, 3, two).wait_send()
    for j in range(4):
        to_near(j).wait_send()
        if j > 0:
            passing(mine, 3 + j, near).wait_send()
    for index, partner in enumerate((two, two, one)):
        hopping(index, partner).wait_send()


def channel_mixer(normed, weights, mixed, gain, overlap):
    share, features = normed.shape
    vmem = pl.BlockSpec(memory_space=pltpu.VMEM)
    block = (share, features)
    return pl.pallas_call(
        functools.partial(ffn_kernel, overlap),
        in_specs=[vmem] * 6,
        out_specs=vmem,
        out_shape=jax.ShapeDtypeStruct(block, BF16),
        scratch_shapes=[
            pltpu.VMEM((8, *block), BF16),
            pltpu.VMEM((4, *block), F32),
            pltpu.VMEM((4, *block), BF16),
            pltpu.VMEM((4, *block), BF16),
            pltpu.VMEM((3, *block), BF16),
            pltpu.VMEM((3, *block), BF16),
            pltpu.SemaphoreType.DMA((7,)),
            pltpu.SemaphoreType.DMA((8,)),
            pltpu.SemaphoreType.DMA((4,)),
            pltpu.SemaphoreType.DMA((4,)),
            pltpu.SemaphoreType.DMA((3,)),
            pltpu.SemaphoreType.DMA((3,)),
        ],
        compiler_params=pltpu.CompilerParams(
            collective_id=1, has_side_effects=True, vmem_limit_bytes=VMEM_BYTES
        ),
        cost_estimate=pl.CostEstimate(
            flops=40_000_000_000, bytes_accessed=share * features, transcendentals=0
        ),
        name="channel_mixer",
    )(normed, *weights, mixed, gain)


def reversed_bits(value, count):
    out = 0
    bit = 1
    while bit < count:
        out = out * 2 + (value // bit) % 2
        bit *= 2
    return out


def scattered(blocks, axis):
    bit = 1
    while True:
        half = blocks.shape[0] // 2
        other = paired(blocks[half:], axis, bit)
        if half == 1:
            return blocks[0], other[0]
        blocks = (blocks[:half].astype(F32) + other.astype(F32)).astype(BF16)
        bit *= 2


def layer(
    residual,
    small_heads,
    large_heads,
    state_keys,
    state_queries,
    small_gate,
    large_gate,
    small_step,
    large_step,
    small_taps,
    large_taps,
    key_taps,
    query_taps,
    small_decay,
    large_decay,
    small_gain,
    large_gain,
    small_out,
    large_out,
    mixer_gain,
    ffn_in_gain,
    gate_proj,
    up_proj,
    down_proj,
    ffn_out_gain,
):
    length, features = residual.shape
    state_len = state_keys.shape[-1]
    key_rows = state_keys.reshape(length, -1)
    query_rows = state_queries.reshape(length, -1)
    halo_rows = small_taps.shape[0] - 1
    first_row = length - halo_rows
    last = jnp.concatenate(
        [a[first_row:] for a in (small_heads, large_heads, key_rows, query_rows)], axis=1
    )
    halo = earlier(last, SEQ, 1)
    halo = jnp.pad(halo, ((HALO - halo_rows, 0), (0, 0)))
    weights = gathered(gate_proj, up_proj, down_proj)

    heads_a = small_step.shape[1]
    heads_b = large_step.shape[1]
    heads = heads_a + heads_b
    width_a = small_heads.shape[1]
    width_b = large_heads.shape[1]
    width = width_a + width_b
    everything = width + key_rows.shape[1] + query_rows.shape[1]
    sizes = ((heads_a, width_a // heads_a), (heads_b, width_b // heads_b), state_len)
    steps = jnp.pad(
        jnp.concatenate([small_step, large_step], axis=1), ((0, 0), (0, SLOTS - heads))
    )
    steps_across = steps.T
    decay = jnp.pad(jnp.concatenate([small_decay, large_decay]), (0, SLOTS - heads))
    taps = jnp.concatenate(
        [
            small_taps,
            large_taps,
            key_taps.reshape(halo_rows + 1, -1),
            query_taps.reshape(halo_rows + 1, -1),
        ],
        axis=1,
    ).astype(F32)
    gain = jnp.concatenate([small_gain, large_gain]).astype(F32)[None]
    blocks = length // BLOCK

    def rows(columns):
        return pl.BlockSpec((BLOCK, columns), lambda i, *_: (i, 0))

    def whole(*shape):
        return pl.BlockSpec(shape, lambda i, *_: (0,) * len(shape))

    conv, packed = pl.pallas_call(
        functools.partial(conv_kernel, sizes),
        grid=(blocks,),
        in_specs=[
            rows(width_a),
            rows(width_b),
            rows(key_rows.shape[1]),
            rows(query_rows.shape[1]),
            whole(HALO, everything),
            whole(halo_rows + 1, everything),
            rows(SLOTS),
            whole(1, SLOTS),
        ],
        out_specs=[rows(everything), whole(state_len + TAIL, width)],
        out_shape=[
            jax.ShapeDtypeStruct((length, everything), BF16),
            jax.ShapeDtypeStruct((state_len + TAIL, width), BF16),
        ],
        scratch_shapes=[
            pltpu.VMEM((HALO, everything), BF16),
            pltpu.VMEM((state_len, width), F32),
            pltpu.VMEM((1, SLOTS), F32),
        ],
        cost_estimate=pl.CostEstimate(
            flops=10_000_000_000, bytes_accessed=length * everything * 4, transcendentals=0
        ),
        name="convolve",
    )(small_heads, large_heads, key_rows, query_rows, halo, taps, steps, decay[None])

    def opened(array):
        whole_log = array[state_len : state_len + 1].astype(F32)
        whole_log = whole_log + array[state_len + 1 : state_len + 2].astype(F32)
        return array[:state_len].astype(F32), whole_log

    count = lax.axis_size(SEQ)
    near = 1
    while near * near < count:
        near *= 2
    received = [opened(earlier(packed, SEQ, d)) for d in range(1, near + 1)]
    entering, log = received[-1]
    for nearer, nearer_log in received[-2::-1]:
        entering = entering * jnp.exp(nearer_log) + nearer
        log = log + nearer_log
    distance = near
    while distance < count:
        high = lax.reduce_precision(log, 8, 7)
        sent = jnp.concatenate(
            [
                entering.astype(BF16),
                high.astype(BF16),
                (log - high).astype(BF16),
            ],
            axis=0,
        )
        far_state, far_log = opened(earlier(sent, SEQ, distance))
        entering = far_state * jnp.exp(log) + entering
        log = log + far_log
        distance *= 2

    share_count = lax.axis_size(HEADS)
    me = lax.axis_index(HEADS)
    share = length // share_count
    per_share = share // BLOCK

    def out_place(i, place):
        return (reversed_bits((i // per_share) ^ place[0], share_count), i % per_share, 0)

    partial_value = pl.pallas_call(
        functools.partial(mix_kernel, sizes),
        grid_spec=pltpu.PrefetchScalarGridSpec(
            num_scalar_prefetch=1,
            grid=(blocks,),
            in_specs=[
                rows(everything),
                rows(width_a),
                rows(width_b),
                rows(SLOTS),
                pl.BlockSpec((SLOTS, BLOCK), lambda i, *_: (0, i)),
                whole(1, SLOTS),
                whole(SLOTS, 1),
                whole(1, width),
                whole(width_a, features),
                whole(width_b, features),
                whole(state_len, width),
            ],
            out_specs=pl.BlockSpec((1, BLOCK, features), out_place),
            scratch_shapes=[pltpu.VMEM((state_len, width), F32)],
        ),
        out_shape=jax.ShapeDtypeStruct((share_count, share, features), BF16),
        cost_estimate=pl.CostEstimate(
            flops=10_000_000_000, bytes_accessed=length * features * 4, transcendentals=0
        ),
        name="mix",
    )(
        jnp.reshape(me, (1,)).astype(jnp.int32),
        conv,
        small_gate,
        large_gate,
        steps,
        steps_across,
        decay[None],
        decay[:, None],
        gain,
        small_out,
        large_out,
        entering,
    )
    mix_one, mix_other = scattered(partial_value, HEADS)
    own = lax.dynamic_slice_in_dim(residual, me * share, share, 0)
    tile = BLOCK // 2

    def strips(columns):
        return pl.BlockSpec((tile, columns), lambda i, *_: (i, 0))

    mixed, normed_own = pl.pallas_call(
        norm_kernel,
        grid=(share // tile,),
        in_specs=[strips(features)] * 3 + [whole(1, features)] * 2,
        out_specs=[strips(features)] * 2,
        out_shape=[
            jax.ShapeDtypeStruct((share, features), F32),
            jax.ShapeDtypeStruct((share, features), BF16),
        ],
        cost_estimate=pl.CostEstimate(
            flops=1_000_000_000, bytes_accessed=share * features * 12, transcendentals=0
        ),
        name="norms",
    )(mix_one, mix_other, own, mixer_gain[None], ffn_in_gain[None])
    columns = gate_proj.shape[1]
    overlap = 2 * half_width(columns) - columns
    return channel_mixer(normed_own, weights, mixed, ffn_out_gain[None], overlap)


def solution(mesh):
    placed = (
        P(SEQ, None),
        P(SEQ, HEADS),
        P(SEQ, HEADS),
        P(SEQ, HEADS, None),
        P(SEQ, HEADS, None),
        P(SEQ, HEADS),
        P(SEQ, HEADS),
        P(SEQ, HEADS),
        P(SEQ, HEADS),
        P(None, HEADS),
        P(None, HEADS),
        P(None, HEADS, None),
        P(None, HEADS, None),
        P(HEADS),
        P(HEADS),
        P(HEADS),
        P(HEADS),
        P(HEADS, None),
        P(HEADS, None),
        P(),
        P(),
        P(SEQ, HEADS),
        P(SEQ, HEADS),
        P(SEQ, HEADS),
        P(),
    )
    outer, heads = mesh.shape["sp"] // 2, mesh.shape["tp"] // 2
    cut = jax.sharding.Mesh(mesh.devices.reshape(outer, 2, heads, 2), (OUTER, INNER, CHIP, CORE))
    return jax.shard_map(
        layer, mesh=cut, in_specs=placed, out_specs=P((*SEQ, *HEADS), None), check_vma=False
    )
```

```python
import functools
import types

import jax
import jax.numpy as jnp
from jax import lax
from jax.experimental import pallas as pl
from jax.experimental.pallas import tpu as pltpu
from jax.sharding import PartitionSpec as P

BLOCK = 128
HALO = 16
LANES = 128
SLOTS = 8
TAIL = 16
CHUNK = 256
RING = 4
AHEAD = 2


EPS = 1e-06
OUTER, INNER = "so", "si"
SEQ = (OUTER, INNER)
CHIP, CORE = "tx", "tc"
HEADS = (CHIP, CORE)
MESH = pl.DeviceIdType.MESH
VMEM_BYTES = 64 * 1024 * 1024 - 128 * 1024
FAR = -1e30
F32 = jnp.float32
BF16 = jnp.bfloat16


def silu(x):
    return x / (1.0 + jnp.exp(-x))


def softplus(x):
    return jnp.maximum(x, 0.0) + jnp.log1p(jnp.exp(-jnp.abs(x)))


def exact_dot(a, b):
    return lax.dot_general(
        a, b, (((1,), (0,)), ((), ())), precision=lax.Precision.HIGHEST, preferred_element_type=F32
    )


def exact_across(a, b):
    return lax.dot_general(
        a, b, (((0,), (0,)), ((), ())), precision=lax.Precision.HIGHEST, preferred_element_type=F32
    )


def lower(n):
    rows = lax.broadcasted_iota(jnp.int32, (n, n), 0)
    return rows >= lax.broadcasted_iota(jnp.int32, (n, n), 1)


def spread(columns, heads, dim):
    rows = columns.shape[0]
    parts = []
    if dim >= LANES:
        for h in heads:
            parts.append(jnp.broadcast_to(columns[:, h : h + 1], (rows, dim)))
    else:
        per = LANES // dim
        lane = lax.broadcasted_iota(jnp.int32, (rows, LANES), 1)
        for first in range(0, len(heads), per):
            part = jnp.broadcast_to(columns[:, heads[first] : heads[first] + 1], (rows, LANES))
            for j in range(1, per):
                h = heads[first + j]
                part = jnp.where(lane >= j * dim, columns[:, h : h + 1], part)
            parts.append(part)
    return jnp.concatenate(parts, axis=1)


def unit_rms(values):
    return values * lax.rsqrt(jnp.mean(values * values, axis=-1, keepdims=True) + EPS)


def flipped(value, by):
    return value + by * (1 - 2 * value)


def half_width(columns):
    return (columns // LANES + 1) // 2 * LANES


def greet(partners):
    barrier = pltpu.get_barrier_semaphore()
    for partner in partners:
        pl.semaphore_signal(barrier, inc=1, device_id=partner, device_id_type=MESH)
    pl.semaphore_wait(barrier, len(partners))


def remote(source, target, send, recv, partner):
    copy = pltpu.make_async_remote_copy(
        src_ref=source,
        dst_ref=target,
        send_sem=send,
        recv_sem=recv,
        device_id=partner,
        device_id_type=MESH,
    )
    return copy


def layer_kernel(names, sizes, overlap, *refs):
    r = types.SimpleNamespace(**dict(zip(names, refs, strict=True)))
    (heads_a, dim_a), (heads_b, dim_b), state_len = sizes
    width_a, width_b = heads_a * dim_a, heads_b * dim_b
    width = width_a + width_b
    groups = (
        (list(range(heads_a)), dim_a, width_a, 0, width),
        (list(range(heads_a, heads_a + heads_b)), dim_b, width_b, width_a, width + state_len),
    )
    length, everything = r.values.shape
    blocks = length // BLOCK
    share, features = r.out.shape
    count = lax.axis_size(OUTER)
    z, y = lax.axis_index(OUTER), lax.axis_index(INNER)
    x, c = lax.axis_index(CHIP), lax.axis_index(CORE)
    pair = z % 2
    first_z = z - pair
    position = 2 * z + y
    side = {INNER: 1 - y}
    near = {CORE: 1 - c}
    across = {CHIP: 1 - x}
    one = {OUTER: z + (1 - c) * (1 - 2 * pair), CHIP: flipped(x, c)}
    two = {OUTER: z + c * (1 - 2 * pair), CHIP: flipped(x, 1 - c)}
    line = [{OUTER: (z + d) % count} for d in range(1, count)]
    turn = [{OUTER: (z + d) % count, INNER: 1 - y} for d in (1, count - 1)]
    greet([side, near, across, *line, *turn])

    inputs = (r.small, r.large, r.keys, r.queries)
    column = 0
    halo_columns = []
    for ref in inputs:
        halo_columns.append(pl.ds(column, ref.shape[1]))
        column += ref.shape[1]

    def halo_copy(index, partner):
        return remote(
            inputs[index].at[pl.ds(length - HALO, HALO)],
            r.halo.at[:, halo_columns[index]],
            r.halo_send.at[index],
            r.halo_recv.at[index],
            partner,
        )

    next_z = (z + 1) % count
    last = position == 2 * count - 1

    @pl.when(y == 0)
    def _():
        for index in range(4):
            halo_copy(index, side).start()

    @pl.when((y == 1) & ~last)
    def _():
        for index in range(4):
            halo_copy(index, {OUTER: next_z, INNER: 0}).start()

    loads = []

    def load(source, target):
        copy = pltpu.make_async_copy(source, target, r.load_sem.at[len(loads)])
        copy.start()
        loads.append(copy)

    for index, ref in enumerate(inputs):
        load(ref, r.values.at[:, halo_columns[index]])

    shards = (r.gate_proj, r.up_proj, r.down_proj)
    gathered = (r.gate_all, r.up_all, r.down_all)
    rows, columns = r.gate_proj.shape
    wide = r.gate_all.shape[1]

    def half(m, member):
        start = pl.multiple_of(member * (columns - wide), LANES)
        return shards[m].at[:, pl.ds(start, wide)]

    def piece(m, source):
        return gathered[m].at[pl.ds(pl.multiple_of((source * 2 + y) * rows, rows), rows)]

    def to_line(m, target):
        return remote(half(m, target % 2), piece(m, z), r.send.at[m, target], r.recv.at[m, z], {OUTER: target})

    def from_line(m, source):
        return remote(piece(m, source), piece(m, source), r.send.at[m, source], r.recv.at[m, source], side)

    def own_side(m):
        return remote(half(m, pair), piece(m, z), r.side_send.at[m, z], r.side_recv.at[m, z], side)

    def relay(m, source):
        return remote(
            piece(m, source), piece(m, source), r.side_send.at[m, source], r.side_recv.at[m, source], side
        )

    mate = first_z + 1 - pair
    sources = [mate] + [(first_z + q) % count for q in range(2, count)]

    def pump(m, source):
        from_line(m, source).wait_recv()
        relay(m, source).start()

    for target in sources:
        to_line(0, target).start()
    for m in range(3):
        own_side(m).start()
        load(half(m, pair), piece(m, z))
    load(r.small_gate, r.gates.at[:, pl.ds(0, width_a)])
    load(r.large_gate, r.gates.at[:, pl.ds(width_a, width_b)])
    load(r.small_out, r.out_rows.at[pl.ds(0, width_a)])
    load(r.large_out, r.out_rows.at[pl.ds(width_a, width_b)])
    me = x * 2 + c
    load(r.residual.at[pl.ds(pl.multiple_of(me * share, share), share)], r.out)

    for index in range(4):
        loads[index].wait()

    @pl.when(position > 0)
    def _():
        for index in range(4):
            halo_copy(index, side).wait_recv()
        r.before[...] = r.halo[...]

    @pl.when(position == 0)
    def _():
        r.before[...] = jnp.zeros_like(r.before)

    r.state[...] = jnp.zeros_like(r.state)
    r.total[...] = jnp.zeros_like(r.total)
    causal = lower(BLOCK)
    ones = causal.astype(F32)
    rates = jnp.exp(r.decay[...])

    def block_rows(i):
        return pl.ds(pl.multiple_of(i * BLOCK, BLOCK), BLOCK)

    def convolve(i, _):
        here_rows = block_rows(i)
        taps_len = r.taps.shape[0]
        for start in range(0, everything, LANES):
            here = pl.ds(start, LANES)
            now = r.values[here_rows, here]
            extended = jnp.concatenate([r.before[:, here], now], axis=0).astype(F32)
            summed = None
            for k in range(taps_len):
                first = HALO - taps_len + 1 + k
                term = r.taps[k : k + 1, here] * extended[first : first + BLOCK]
                summed = term if summed is None else summed + term
            r.before[:, here] = now[BLOCK - HALO :]
            r.values[here_rows, here] = silu(summed).astype(BF16)
        dt = softplus(r.steps[here_rows])
        cum = exact_dot(ones, -dt * rates)
        tail = cum[BLOCK - 1 : BLOCK]
        scale = dt * jnp.exp(tail - cum)
        kept = jnp.exp(tail)
        r.logs[here_rows] = r.total[...] + cum
        r.total[...] = r.total[...] + tail
        for heads, dim, size, offset, key_at in groups:
            columns_here = pl.ds(offset, size)
            values = r.values[here_rows, columns_here].astype(F32)
            u = (values * spread(scale, heads, dim)).astype(BF16)
            k = r.values[here_rows, pl.ds(key_at, state_len)]
            fresh = lax.dot_general(k, u, (((0,), (0,)), ((), ())), preferred_element_type=F32)
            old = r.state[:, columns_here]
            r.states[i, :, columns_here] = old.astype(BF16)
            r.state[:, columns_here] = old * spread(kept, heads, dim) + fresh
        return 0

    lax.fori_loop(0, blocks, convolve, 0)

    def pack(target, state, log):
        target[:state_len] = state.astype(BF16)
        high = log.astype(BF16)
        low = (log - high.astype(F32)).astype(BF16)
        row = lax.broadcasted_iota(jnp.int32, (TAIL, width), 0)
        both = jnp.where(row == 0, high.astype(F32), jnp.where(row == 1, low.astype(F32), 0.0))
        target[state_len:] = both.astype(BF16)

    def opened(ref):
        tail = ref[state_len:].astype(F32)
        return ref[:state_len].astype(F32), tail[0:1] + tail[1:2]

    pack(
        r.packed,
        r.state[...],
        jnp.concatenate([spread(r.total[...], heads, dim) for heads, dim, *_ in groups], axis=1),
    )
    pair_copy = remote(r.packed, r.beside, r.state_send.at[0], r.state_recv.at[0], side)
    pair_copy.start()
    for target in sources:
        to_line(1, target).start()

    upper = (
        lax.broadcasted_iota(jnp.int32, (BLOCK, BLOCK), 0)
        <= lax.broadcasted_iota(jnp.int32, (BLOCK, BLOCK), 1)
    ).astype(F32)
    same = (
        lax.broadcasted_iota(jnp.int32, (BLOCK, BLOCK), 0)
        == lax.broadcasted_iota(jnp.int32, (BLOCK, BLOCK), 1)
    ).astype(F32)
    lane = lax.broadcasted_iota(jnp.int32, (BLOCK, LANES), 1)

    def inside_block(i, _):
        here_rows = block_rows(i)
        dt = softplus(r.steps[here_rows])
        log = -dt * rates
        cum = exact_dot(ones, log)
        cum_across = exact_across(log, upper)
        dt_across = exact_across(dt, same)
        grown = jnp.exp(cum)
        for heads, dim, size, offset, key_at in groups:
            columns_here = pl.ds(offset, size)
            values = r.values[here_rows, columns_here]
            k = r.values[here_rows, pl.ds(key_at, state_len)]
            q = r.values[here_rows, pl.ds(key_at + 2 * state_len, state_len)]
            scores = lax.dot_general(q, k, (((1,), (1,)), ((), ())), preferred_element_type=F32)
            carried = jnp.dot(q, r.states[i, :, columns_here], preferred_element_type=F32)
            carried = carried * spread(grown, heads, dim)
            inside = []
            span = max(dim, LANES)
            per = span // dim
            for first in range(0, len(heads), per):
                part_values = values[:, first * dim : first * dim + span]
                part = None
                for j in range(per):
                    h = heads[first + j]
                    gap = cum[:, h : h + 1] - cum_across[h : h + 1]
                    decays = jnp.exp(jnp.where(causal, gap, FAR))
                    w = (scores * decays * dt_across[h : h + 1]).astype(BF16)
                    got = jnp.dot(w, part_values, preferred_element_type=F32)
                    part = got if part is None else jnp.where(lane >= j * dim, got, part)
                inside.append(part)
            r.inner[here_rows, columns_here] = jnp.concatenate(inside, axis=1) + carried
        return 0

    lax.fori_loop(0, blocks // 2, inside_block, 0)

    pair_copy.wait_recv()
    mine, mine_log = opened(r.packed)
    theirs, theirs_log = opened(r.beside)
    front = y == 0
    lead = jnp.where(front, mine, theirs)
    lead_log = jnp.where(front, mine_log, theirs_log)
    trail = jnp.where(front, theirs, mine)
    trail_log = jnp.where(front, theirs_log, mine_log)
    r.both[:state_len] = lead * jnp.exp(trail_log) + trail
    r.both[state_len:] = jnp.broadcast_to(lead_log + trail_log, (8, width))
    r.ahead[:state_len] = lead
    r.ahead[state_len:] = jnp.broadcast_to(lead_log, (8, width))

    def line_copy():
        return remote(r.passed, r.arrived, r.state_send.at[1], r.state_recv.at[1], {OUTER: next_z})

    @pl.when(z == 0)
    def _():
        pack(r.passed, r.both[:state_len], r.both[state_len : state_len + 1])
        line_copy().start()

    lax.fori_loop(blocks // 2, blocks, inside_block, 0)

    @pl.when(z == 0)
    def _():
        r.state[...] = jnp.zeros_like(r.state)

    @pl.when(z > 0)
    def _():
        line_copy().wait_recv()
        before, before_log = opened(r.arrived)
        r.state[...] = before

        @pl.when(z < count - 1)
        def _():
            both_log = r.both[state_len : state_len + 1]
            pack(r.passed, before * jnp.exp(both_log) + r.both[:state_len], before_log + both_log)
            line_copy().start()

    @pl.when(y == 1)
    def _():
        r.state[...] = r.state[...] * jnp.exp(r.ahead[state_len : state_len + 1]) + r.ahead[:state_len]

    r.entering[...] = r.state[...].astype(BF16)
    for target in sources:
        to_line(2, target).start()
    queue = [(m, source) for m in range(2) for source in sources]
    marks = [len(queue) * k // 6 for k in range(7)]

    def pumps(first, end):
        for m, source in queue[marks[first] : marks[end]]:
            pump(m, source)

    pumps(0, 2)
    for index in range(7, len(loads)):
        loads[index].wait()

    def near_mix(index):
        return remote(
            r.mix_core.at[index], r.mix_from.at[index], r.mix_send.at[index], r.mix_recv.at[index], near
        )

    across_mix = remote(r.mix_hop, r.mix_got, r.mix_send.at[2], r.mix_recv.at[2], across)

    per_share = share // BLOCK

    def project(b, _):
        which = b // per_share
        far, other = 1 - which // 2, 1 - which % 2
        source = flipped(x, far) * 2 + flipped(c, other)
        i = source * per_share + b % per_share
        here_rows = block_rows(i)
        grown = jnp.exp(r.logs[here_rows])
        result = None
        for heads, dim, size, offset, key_at in groups:
            columns_here = pl.ds(offset, size)
            q = r.values[here_rows, pl.ds(key_at + 2 * state_len, state_len)]
            carried = jnp.dot(q, r.entering[:, columns_here], preferred_element_type=F32)
            mixed = r.inner[here_rows, columns_here] + carried * spread(grown, heads, dim)
            gated = mixed * silu(r.gates[here_rows, columns_here].astype(F32))
            squares = gated * gated
            span = max(dim, LANES)
            per = span // dim
            normed = []
            for first in range(0, len(heads), per):
                at = first * dim
                part = squares[:, at : at + span]
                means = None
                for j in range(per):
                    if per == 1:
                        means = jnp.sum(part, axis=1, keepdims=True)
                    else:
                        ours = (lane >= j * dim) & (lane < (j + 1) * dim)
                        single = jnp.sum(jnp.where(ours, part, 0.0), axis=1, keepdims=True)
                        means = single if means is None else jnp.where(lane >= j * dim, single, means)
                normed.append(gated[:, at : at + span] * lax.rsqrt(means * (1.0 / dim) + EPS))
            normed = jnp.concatenate(normed, axis=1) * r.gain[:, columns_here]
            product = jnp.dot(normed.astype(BF16), r.out_rows[columns_here], preferred_element_type=F32)
            result = product if result is None else result + product
        part_rows = pl.ds(pl.multiple_of(b % per_share * BLOCK, BLOCK), BLOCK)

        @pl.when(other == 1)
        def _():
            r.mix_core[far, part_rows] = result.astype(BF16)

        @pl.when(other == 0)
        def _():
            r.mix_local[far, part_rows] = result

        @pl.when((other == 1) & (b % per_share == per_share - 1))
        def _():
            near_mix(far).start()

        @pl.when(b == 2 * per_share - 1)
        def _():
            near_mix(1).wait_recv()
            r.mix_hop[...] = (r.mix_local[1] + r.mix_from[1].astype(F32)).astype(BF16)
            across_mix.start()

        return 0

    lax.fori_loop(0, blocks, project, 0)
    pumps(2, 4)
    near_mix(0).wait_recv()
    across_mix.wait_recv()

    def place(core, d_one, d_two):
        dz = d_one * (1 - core) + d_two * core
        dx = d_one * core + d_two * (1 - core)
        return (flipped(pair, dz) * 2 + flipped(x, dx)) * 2 + core

    mine_at = place(c, 0, 0)
    tile = BLOCK // 2

    def norms(i, _):
        here = pl.ds(pl.multiple_of(i * tile, tile), tile)
        mix = r.mix_local[0, here] + r.mix_from[0, here].astype(F32) + r.mix_got[here].astype(F32)
        mixed = r.out[here].astype(F32) + unit_rms(mix) * r.gains[0:1]
        r.mixed[here] = mixed
        r.rows[mine_at, here] = (unit_rms(mixed) * r.gains[1:2]).astype(BF16)
        return 0

    lax.fori_loop(0, share // tile, norms, 0)

    def passing(slot, index, partner):
        return remote(r.rows.at[slot], r.rows.at[slot], r.rows_send.at[index], r.rows_recv.at[slot], partner)

    for index, partner in enumerate((one, two, near)):
        passing(mine_at, index, partner).start()
    pumps(4, 6)
    for m in range(2):
        loads[4 + m].wait()
        for source in range(count):
            relay(m, source).wait_recv()

    def hidden_of(slot):
        values = r.rows[slot]
        gate = jnp.dot(values, r.gate_all[...], preferred_element_type=F32)
        up = jnp.dot(values, r.up_all[...], preferred_element_type=F32)
        hidden = silu(gate) * up
        at = lax.broadcasted_iota(jnp.int32, hidden.shape, 1)
        return jnp.where(at >= pair * overlap, hidden, 0.0).astype(BF16)

    def expand(j, _):
        d_one, d_two = j % 2, j // 2
        slot = place(c, d_one, d_two)

        @pl.when(j > 0)
        def _():
            passing(slot, 0, near).wait_recv()
            passing(slot, 3 + j, near).start()

        @pl.when(j == 1)
        def _():
            passing(slot, 3, two).start()

        r.hidden[j] = hidden_of(slot)
        slot = place(1 - c, d_one, d_two)
        passing(slot, 0, near).wait_recv()
        r.hidden[4 + j] = hidden_of(slot)
        return 0

    lax.fori_loop(0, 4, expand, 0)

    chunk = r.got_one.shape[-1]
    per_chunk = chunk // rows
    chunks = features // chunk
    first_chunk = 2 * first_z * rows // chunk

    def chunk_at(k):
        return (first_chunk + k) % chunks

    def pump_chunk(k):
        for index in range(per_chunk):
            block = chunk_at(k) * per_chunk + index

            @pl.when((block % 2 == y) & (block // 2 != z))
            def _():
                pump(2, block // 2)

    def near_copy(k):
        return remote(
            r.to_core.at[k % RING], r.from_core.at[k], r.core_send.at[k % RING], r.core_recv.at[k], near
        )

    def two_copy(k):
        return remote(r.hop_two.at[k % RING], r.got_two.at[k], r.two_send.at[k % RING], r.two_recv.at[k], two)

    def one_copy(k):
        return remote(r.hop_one.at[k % RING], r.got_one.at[k], r.one_send.at[k % RING], r.one_recv.at[k], one)

    def local_at(k, j):
        slot = k % RING
        start = pl.multiple_of((slot % 2 * 4 + j) * chunk, LANES)
        return slot // 2, slice(None), pl.ds(start, chunk)

    loads[6].wait()
    for k in range(AHEAD):
        pump_chunk(k)

    def reduce_step(k, _):
        @pl.when(k < chunks)
        def _():
            for index in range(per_chunk):
                block = chunk_at(k) * per_chunk + index

                @pl.when(block % 2 != y)
                def _():
                    relay(2, block // 2).wait_recv()

            @pl.when(k >= RING)
            def _():
                near_copy(k).wait_send()

            at = pl.ds(pl.multiple_of(chunk_at(k) * chunk, chunk), chunk)
            weights = r.down_all[at]
            for j in range(4):
                r.to_core[k % RING, j] = lax.dot_general(
                    r.hidden[4 + j], weights, (((1,), (1,)), ((), ())), preferred_element_type=F32
                ).astype(BF16)
            near_copy(k).start()
            for j in range(4):
                r.mix_local[local_at(k, j)] = lax.dot_general(
                    r.hidden[j], weights, (((1,), (1,)), ((), ())), preferred_element_type=F32
                )

        @pl.when((k >= 1) & (k < chunks + 1))
        def _():
            p = k - 1
            near_copy(p).wait_recv()

            @pl.when(p >= RING)
            def _():
                two_copy(p).wait_send()

            for index, j in enumerate((3, 2)):
                total = r.mix_local[local_at(p, j)] + r.from_core[p, j].astype(F32)
                r.hop_two[p % RING, index] = total.astype(BF16)
            two_copy(p).start()
            for j in range(2):
                r.mix_local[local_at(p, j)] = r.mix_local[local_at(p, j)] + r.from_core[p, j].astype(F32)

        @pl.when((k >= 2) & (k < chunks + 2))
        def _():
            p = k - 2
            two_copy(p).wait_recv()

            @pl.when(p >= RING)
            def _():
                one_copy(p).wait_send()

            total = r.mix_local[local_at(p, 1)] + r.got_two[p, 0].astype(F32)
            r.hop_one[p % RING] = total.astype(BF16)
            one_copy(p).start()

        @pl.when(k >= 3)
        def _():
            p = k - 3
            one_copy(p).wait_recv()
            total = r.mix_local[local_at(p, 0)] + r.got_two[p, 1].astype(F32) + r.got_one[p].astype(F32)
            r.ffn[:, pl.ds(pl.multiple_of(chunk_at(p) * chunk, chunk), chunk)] = total

        @pl.when(k < chunks - AHEAD)
        def _():
            pump_chunk(k + AHEAD)

        return 0

    lax.fori_loop(0, chunks + 3, reduce_step, 0)

    def finish(i, _):
        here = pl.ds(pl.multiple_of(i * tile, tile), tile)
        r.out[here] = (r.mixed[here] + 0.5 * unit_rms(r.ffn[here]) * r.gains[2:3]).astype(BF16)
        return 0

    lax.fori_loop(0, share // tile, finish, 0)

    @pl.when(~last)
    def _():
        for index in range(4):
            halo_copy(index, side).wait_send()

    pair_copy.wait_send()

    @pl.when(z < count - 1)
    def _():
        line_copy().wait_send()

    for m in range(3):
        for target in sources:
            to_line(m, target).wait_send()
        for source in range(count):
            relay(m, source).wait_send()
    near_mix(0).wait_send()
    near_mix(1).wait_send()
    across_mix.wait_send()
    for index in range(7):
        passing(mine_at, index, near).wait_send()
    for slot in range(min(RING, chunks)):
        near_copy(slot).wait_send()
        two_copy(slot).wait_send()
        one_copy(slot).wait_send()


def layer(
    residual,
    small_heads,
    large_heads,
    state_keys,
    state_queries,
    small_gate,
    large_gate,
    small_step,
    large_step,
    small_taps,
    large_taps,
    key_taps,
    query_taps,
    small_decay,
    large_decay,
    small_gain,
    large_gain,
    small_out,
    large_out,
    mixer_gain,
    ffn_in_gain,
    gate_proj,
    up_proj,
    down_proj,
    ffn_out_gain,
):
    length, features = residual.shape
    state_len = state_keys.shape[-1]
    key_rows = state_keys.reshape(length, -1)
    query_rows = state_queries.reshape(length, -1)
    heads_a = small_step.shape[1]
    heads_b = large_step.shape[1]
    heads = heads_a + heads_b
    width_a = small_heads.shape[1]
    width_b = large_heads.shape[1]
    width = width_a + width_b
    everything = width + key_rows.shape[1] + query_rows.shape[1]
    sizes = ((heads_a, width_a // heads_a), (heads_b, width_b // heads_b), state_len)
    steps = jnp.pad(
        jnp.concatenate([small_step, large_step], axis=1), ((0, 0), (0, SLOTS - heads))
    )
    decay = jnp.pad(jnp.concatenate([small_decay, large_decay]), (0, SLOTS - heads))
    taps_len = small_taps.shape[0]
    taps = jnp.concatenate(
        [small_taps, large_taps, key_taps.reshape(taps_len, -1), query_taps.reshape(taps_len, -1)],
        axis=1,
    ).astype(F32)
    gain = jnp.concatenate([small_gain, large_gain]).astype(F32)[None]
    gains = jnp.stack([mixer_gain, ffn_in_gain, ffn_out_gain]).astype(F32)
    share = length // lax.axis_size(HEADS)
    rows, columns = down_proj.shape
    count = lax.axis_size(OUTER)
    wide = half_width(columns)
    chunk = max(rows, CHUNK)
    chunks = features // chunk
    blocks = length // BLOCK
    vmem = pl.BlockSpec(memory_space=pltpu.VMEM)
    hbm = pl.BlockSpec(memory_space=pl.ANY)
    dma = pltpu.SemaphoreType.DMA
    operands = {
        "small": (small_heads, hbm),
        "large": (large_heads, hbm),
        "keys": (key_rows, hbm),
        "queries": (query_rows, hbm),
        "small_gate": (small_gate, hbm),
        "large_gate": (large_gate, hbm),
        "small_out": (small_out, hbm),
        "large_out": (large_out, hbm),
        "residual": (residual, hbm),
        "gate_proj": (gate_proj, hbm),
        "up_proj": (up_proj, hbm),
        "down_proj": (down_proj, hbm),
        "steps": (steps, vmem),
        "decay": (decay[None], vmem),
        "taps": (taps, vmem),
        "gain": (gain, vmem),
        "gains": (gains, vmem),
    }
    packed = (state_len + TAIL, width)
    opened = (state_len + 8, width)
    scratch = {
        "values": pltpu.VMEM((length, everything), BF16),
        "gates": pltpu.VMEM((length, width), BF16),
        "out_rows": pltpu.VMEM((width, features), BF16),
        "gate_all": pltpu.VMEM((features, wide), BF16),
        "up_all": pltpu.VMEM((features, wide), BF16),
        "down_all": pltpu.VMEM((features, wide), BF16),
        "halo": pltpu.VMEM((HALO, everything), BF16),
        "before": pltpu.VMEM((HALO, everything), BF16),
        "state": pltpu.VMEM((state_len, width), F32),
        "states": pltpu.VMEM((blocks, state_len, width), BF16),
        "total": pltpu.VMEM((1, SLOTS), F32),
        "logs": pltpu.VMEM((length, SLOTS), F32),
        "inner": pltpu.VMEM((length, width), F32),
        "packed": pltpu.VMEM(packed, BF16),
        "beside": pltpu.VMEM(packed, BF16),
        "passed": pltpu.VMEM(packed, BF16),
        "arrived": pltpu.VMEM(packed, BF16),
        "both": pltpu.VMEM(opened, F32),
        "ahead": pltpu.VMEM(opened, F32),
        "entering": pltpu.VMEM((state_len, width), BF16),
        "mix_core": pltpu.VMEM((2, share, features), BF16),
        "mix_from": pltpu.VMEM((2, share, features), BF16),
        "mix_local": pltpu.VMEM((2, share, features), F32),
        "mix_hop": pltpu.VMEM((share, features), BF16),
        "mix_got": pltpu.VMEM((share, features), BF16),
        "mixed": pltpu.VMEM((share, features), F32),
        "rows": pltpu.VMEM((8, share, features), BF16),
        "hidden": pltpu.VMEM((8, share, wide), BF16),
        "to_core": pltpu.VMEM((RING, 4, share, chunk), BF16),
        "from_core": pltpu.VMEM((chunks, 4, share, chunk), BF16),
        "hop_two": pltpu.VMEM((RING, 2, share, chunk), BF16),
        "got_two": pltpu.VMEM((chunks, 2, share, chunk), BF16),
        "hop_one": pltpu.VMEM((RING, share, chunk), BF16),
        "got_one": pltpu.VMEM((chunks, share, chunk), BF16),
        "ffn": pltpu.VMEM((share, features), F32),
        "halo_send": dma((4,)),
        "halo_recv": dma((4,)),
        "load_sem": dma((12,)),
        "send": dma((3, count)),
        "recv": dma((3, count)),
        "side_send": dma((3, count)),
        "side_recv": dma((3, count)),
        "state_send": dma((2,)),
        "state_recv": dma((2,)),
        "mix_send": dma((3,)),
        "mix_recv": dma((3,)),
        "rows_send": dma((7,)),
        "rows_recv": dma((8,)),
        "core_send": dma((RING,)),
        "core_recv": dma((chunks,)),
        "two_send": dma((RING,)),
        "two_recv": dma((chunks,)),
        "one_send": dma((RING,)),
        "one_recv": dma((chunks,)),
    }
    names = (*operands, "out", *scratch)
    return pl.pallas_call(
        functools.partial(layer_kernel, names, sizes, 2 * wide - columns),
        in_specs=[spec for _, spec in operands.values()],
        out_specs=vmem,
        out_shape=jax.ShapeDtypeStruct((share, features), BF16),
        scratch_shapes=list(scratch.values()),
        compiler_params=pltpu.CompilerParams(
            collective_id=0, has_side_effects=True, vmem_limit_bytes=VMEM_BYTES
        ),
        cost_estimate=pl.CostEstimate(
            flops=40_000_000_000, bytes_accessed=share * features, transcendentals=0
        ),
        name="layer",
    )(*[array for array, _ in operands.values()])


def solution(mesh):
    placed = (
        P(SEQ, None),
        P(SEQ, HEADS),
        P(SEQ, HEADS),
        P(SEQ, HEADS, None),
        P(SEQ, HEADS, None),
        P(SEQ, HEADS),
        P(SEQ, HEADS),
        P(SEQ, HEADS),
        P(SEQ, HEADS),
        P(None, HEADS),
        P(None, HEADS),
        P(None, HEADS, None),
        P(None, HEADS, None),
        P(HEADS),
        P(HEADS),
        P(HEADS),
        P(HEADS),
        P(HEADS, None),
        P(HEADS, None),
        P(),
        P(),
        P(SEQ, HEADS),
        P(SEQ, HEADS),
        P(SEQ, HEADS),
        P(),
    )
    outer, heads = mesh.shape["sp"] // 2, mesh.shape["tp"] // 2
    cut = jax.sharding.Mesh(mesh.devices.reshape(outer, 2, heads, 2), (OUTER, INNER, CHIP, CORE))
    return jax.shard_map(
        layer, mesh=cut, in_specs=placed, out_specs=P((*SEQ, *HEADS), None), check_vma=False
    )
```

```python
import functools
import types

import jax
import jax.numpy as jnp
from jax import lax
from jax.experimental import pallas as pl
from jax.experimental.pallas import tpu as pltpu
from jax.sharding import PartitionSpec as P

BLOCK = 128
HALO = 16
LANES = 128
SLOTS = 8
TAIL = 16
CHUNK = 256
RING = 4
AHEAD = 3


EPS = 1e-06
OUTER, INNER = "so", "si"
SEQ = (OUTER, INNER)
CHIP, CORE = "tx", "tc"
HEADS = (CHIP, CORE)
MESH = pl.DeviceIdType.MESH
VMEM_BYTES = 64 * 1024 * 1024 - 128 * 1024
FAR = -1e30
F32 = jnp.float32
BF16 = jnp.bfloat16


def silu(x):
    return x / (1.0 + jnp.exp(-x))


def softplus(x):
    return jnp.maximum(x, 0.0) + jnp.log1p(jnp.exp(-jnp.abs(x)))


def exact_dot(a, b):
    return lax.dot_general(
        a, b, (((1,), (0,)), ((), ())), precision=lax.Precision.HIGHEST, preferred_element_type=F32
    )


def exact_across(a, b):
    return lax.dot_general(
        a, b, (((0,), (0,)), ((), ())), precision=lax.Precision.HIGHEST, preferred_element_type=F32
    )


def lower(n):
    rows = lax.broadcasted_iota(jnp.int32, (n, n), 0)
    return rows >= lax.broadcasted_iota(jnp.int32, (n, n), 1)


def spread(columns, heads, dim):
    rows = columns.shape[0]
    parts = []
    if dim >= LANES:
        for h in heads:
            parts.append(jnp.broadcast_to(columns[:, h : h + 1], (rows, dim)))
    else:
        per = LANES // dim
        lane = lax.broadcasted_iota(jnp.int32, (rows, LANES), 1)
        for first in range(0, len(heads), per):
            part = jnp.broadcast_to(columns[:, heads[first] : heads[first] + 1], (rows, LANES))
            for j in range(1, per):
                h = heads[first + j]
                part = jnp.where(lane >= j * dim, columns[:, h : h + 1], part)
            parts.append(part)
    return jnp.concatenate(parts, axis=1)


def unit_rms(values):
    return values * lax.rsqrt(jnp.mean(values * values, axis=-1, keepdims=True) + EPS)


def flipped(value, by):
    return value + by * (1 - 2 * value)


def half_width(columns):
    return (columns // LANES + 1) // 2 * LANES


def greet(partners):
    barrier = pltpu.get_barrier_semaphore()
    for partner in partners:
        pl.semaphore_signal(barrier, inc=1, device_id=partner, device_id_type=MESH)
    pl.semaphore_wait(barrier, len(partners))


def remote(source, target, send, recv, partner):
    copy = pltpu.make_async_remote_copy(
        src_ref=source,
        dst_ref=target,
        send_sem=send,
        recv_sem=recv,
        device_id=partner,
        device_id_type=MESH,
    )
    return copy


def layer_kernel(names, sizes, overlap, *refs):
    r = types.SimpleNamespace(**dict(zip(names, refs, strict=True)))
    (heads_a, dim_a), (heads_b, dim_b), state_len = sizes
    width_a, width_b = heads_a * dim_a, heads_b * dim_b
    width = width_a + width_b
    groups = (
        (list(range(heads_a)), dim_a, width_a, 0, width),
        (list(range(heads_a, heads_a + heads_b)), dim_b, width_b, width_a, width + state_len),
    )
    length, everything = r.values.shape
    blocks = length // BLOCK
    share, features = r.out.shape
    count = lax.axis_size(OUTER)
    z, y = lax.axis_index(OUTER), lax.axis_index(INNER)
    x, c = lax.axis_index(CHIP), lax.axis_index(CORE)
    pair = z % 2
    first_z = z - pair
    position = 2 * z + y
    side = {INNER: 1 - y}
    near = {CORE: 1 - c}
    across = {CHIP: 1 - x}
    upright = {OUTER: first_z + 1 - pair}
    one = {OUTER: z + (1 - c) * (1 - 2 * pair), CHIP: flipped(x, c)}
    two = {OUTER: z + c * (1 - 2 * pair), CHIP: flipped(x, 1 - c)}
    line = [{OUTER: (z + d) % count} for d in range(1, count)]
    turn = [{OUTER: (z + d) % count, INNER: 1 - y} for d in (1, count - 1)]
    greet([side, near, across, *line, *turn])

    inputs = (r.small, r.large, r.keys, r.queries)
    column = 0
    halo_columns = []
    for ref in inputs:
        halo_columns.append(pl.ds(column, ref.shape[1]))
        column += ref.shape[1]

    def halo_copy(index, partner):
        return remote(
            inputs[index].at[pl.ds(length - HALO, HALO)],
            r.halo.at[:, halo_columns[index]],
            r.halo_send.at[index],
            r.halo_recv.at[index],
            partner,
        )

    next_z = (z + 1) % count
    last = position == 2 * count - 1

    @pl.when(y == 0)
    def _():
        for index in range(4):
            halo_copy(index, side).start()

    @pl.when((y == 1) & ~last)
    def _():
        for index in range(4):
            halo_copy(index, {OUTER: next_z, INNER: 0}).start()

    loads = []

    def load(source, target):
        copy = pltpu.make_async_copy(source, target, r.load_sem.at[len(loads)])
        copy.start()
        loads.append(copy)

    for index, ref in enumerate(inputs):
        load(ref, r.values.at[:, halo_columns[index]])

    for index in range(4):
        loads[index].wait()

    @pl.when(position > 0)
    def _():
        for index in range(4):
            halo_copy(index, side).wait_recv()
        r.before[...] = r.halo[...]

    @pl.when(position == 0)
    def _():
        r.before[...] = jnp.zeros_like(r.before)

    shards = (r.gate_proj, r.up_proj, r.down_proj)
    gathered = (r.gate_all, r.up_all, r.down_all)
    rows, columns = r.gate_proj.shape
    wide = r.gate_all.shape[1]

    def half(m, member):
        start = pl.multiple_of(member * (columns - wide), LANES)
        return shards[m].at[:, pl.ds(start, wide)]

    def piece(m, source):
        return gathered[m].at[pl.ds(pl.multiple_of((source * 2 + y) * rows, rows), rows)]

    def to_line(m, target):
        return remote(half(m, target % 2), piece(m, z), r.send.at[m, target], r.recv.at[m, z], {OUTER: target})

    def from_line(m, source):
        return remote(piece(m, source), piece(m, source), r.send.at[m, source], r.recv.at[m, source], side)

    def own_side(m):
        return remote(half(m, pair), piece(m, z), r.side_send.at[m, z], r.side_recv.at[m, z], side)

    def relay(m, source):
        return remote(
            piece(m, source), piece(m, source), r.side_send.at[m, source], r.side_recv.at[m, source], side
        )

    mate = first_z + 1 - pair
    lowest = (count - first_z) // count
    crossing = [lowest * (count + 1 - q) + (1 - lowest) * ((first_z + q) % count) for q in range(2, count)]
    sources = [*crossing[:1], mate, *crossing[1:]]
    edge = (z == 0) | (z == count - 1)

    def pump(m, source):
        from_line(m, source).wait_recv()
        relay(m, source).start()

    def start_line(condition, *pieces):
        @pl.when(condition)
        def _():
            for m, target in pieces:
                to_line(m, target).start()

    outward = [[(m, target) for target in crossing] for m in range(3)]
    both_outward = [*outward[0], *outward[1]]
    rest = [*outward[0][1:], (0, mate), (1, mate)]
    rising = (pair == 0) & ~edge
    falling = (pair == 1) & ~edge
    start_line(edge, outward[0][0])
    start_line(z == count - 1, *rest, *outward[1])
    start_line(falling, (0, mate), (1, mate))
    start_line(rising, *both_outward)
    queue = [(0, crossing[0]), (0, mate), (1, mate)]
    queue += [(0, source) for source in crossing[1:]] + [(1, source) for source in crossing]
    marks = [len(queue) * k // 6 for k in range(7)]

    def pumps(first, end):
        for m, source in queue[marks[first] : marks[end]]:
            pump(m, source)

    own_side(0).start()
    for m in range(3):
        load(half(m, pair), piece(m, z))
    load(r.small_gate, r.gates.at[:, pl.ds(0, width_a)])
    load(r.large_gate, r.gates.at[:, pl.ds(width_a, width_b)])
    load(r.small_out, r.out_rows.at[pl.ds(0, width_a)])
    load(r.large_out, r.out_rows.at[pl.ds(width_a, width_b)])
    me = x * 2 + c
    load(r.residual.at[pl.ds(pl.multiple_of(me * share, share), share)], r.out)

    r.taps[:, pl.ds(0, width_a)] = r.small_taps[...].astype(F32)
    r.taps[:, pl.ds(width_a, width_b)] = r.large_taps[...].astype(F32)
    column = width
    for ref in (r.key_taps, r.query_taps):
        for group in range(ref.shape[1]):
            for k in range(ref.shape[0]):
                r.taps[k : k + 1, pl.ds(column, state_len)] = ref[k, group : group + 1].astype(F32)
            column += state_len
    r.gain[0:1, pl.ds(0, width_a)] = r.small_gain[...].astype(F32)[None]
    r.gain[0:1, pl.ds(width_a, width_b)] = r.large_gain[...].astype(F32)[None]
    for index, ref in enumerate((r.mixer_gain, r.ffn_in_gain, r.ffn_out_gain)):
        r.gains[index : index + 1] = ref[...].astype(F32)[None]
    lanes = lax.broadcasted_iota(jnp.int32, (1, SLOTS), 1)
    decay = jnp.zeros((1, SLOTS), F32)
    for first, heads, ref in ((0, heads_a, r.small_decay), (heads_a, heads_b, r.large_decay)):
        for h in range(heads):
            decay = jnp.where(lanes == first + h, ref[h], decay)

    r.state[...] = jnp.zeros_like(r.state)
    r.total[...] = jnp.zeros_like(r.total)
    causal = lower(BLOCK)
    ones = causal.astype(F32)
    rates = jnp.exp(decay)

    def block_rows(i):
        return pl.ds(pl.multiple_of(i * BLOCK, BLOCK), BLOCK)

    def convolve(i, _):
        here_rows = block_rows(i)
        taps_len = r.taps.shape[0]
        for start in range(0, everything, LANES):
            here = pl.ds(start, LANES)
            now = r.values[here_rows, here]
            extended = jnp.concatenate([r.before[:, here], now], axis=0).astype(F32)
            summed = None
            for k in range(taps_len):
                first = HALO - taps_len + 1 + k
                term = r.taps[k : k + 1, here] * extended[first : first + BLOCK]
                summed = term if summed is None else summed + term
            r.before[:, here] = now[BLOCK - HALO :]
            r.values[here_rows, here] = silu(summed).astype(BF16)
        dt = softplus(r.steps[here_rows])
        cum = exact_dot(ones, -dt * rates)
        tail = cum[BLOCK - 1 : BLOCK]
        scale = dt * jnp.exp(tail - cum)
        kept = jnp.exp(tail)
        r.logs[here_rows] = r.total[...] + cum
        r.total[...] = r.total[...] + tail
        for heads, dim, size, offset, key_at in groups:
            columns_here = pl.ds(offset, size)
            values = r.values[here_rows, columns_here].astype(F32)
            u = (values * spread(scale, heads, dim)).astype(BF16)
            k = r.values[here_rows, pl.ds(key_at, state_len)]
            fresh = lax.dot_general(k, u, (((0,), (0,)), ((), ())), preferred_element_type=F32)
            old = r.state[:, columns_here]
            r.states[i, :, columns_here] = old.astype(BF16)
            r.state[:, columns_here] = old * spread(kept, heads, dim) + fresh
        return 0

    lax.fori_loop(0, blocks, convolve, 0)

    def pack(target, state, log):
        target[:state_len] = state.astype(BF16)
        high = log.astype(BF16)
        low = (log - high.astype(F32)).astype(BF16)
        row = lax.broadcasted_iota(jnp.int32, (TAIL, width), 0)
        both = jnp.where(row == 0, high.astype(F32), jnp.where(row == 1, low.astype(F32), 0.0))
        target[state_len:] = both.astype(BF16)

    def opened(ref):
        tail = ref[state_len:].astype(F32)
        return ref[:state_len].astype(F32), tail[0:1] + tail[1:2]

    pack(
        r.packed,
        r.state[...],
        jnp.concatenate([spread(r.total[...], heads, dim) for heads, dim, *_ in groups], axis=1),
    )
    pair_copy = remote(r.packed, r.beside, r.state_send.at[0], r.state_recv.at[0], side)
    pair_copy.start()
    own_side(1).start()

    upper = (
        lax.broadcasted_iota(jnp.int32, (BLOCK, BLOCK), 0)
        <= lax.broadcasted_iota(jnp.int32, (BLOCK, BLOCK), 1)
    ).astype(F32)
    same = (
        lax.broadcasted_iota(jnp.int32, (BLOCK, BLOCK), 0)
        == lax.broadcasted_iota(jnp.int32, (BLOCK, BLOCK), 1)
    ).astype(F32)
    lane = lax.broadcasted_iota(jnp.int32, (BLOCK, LANES), 1)

    def inside_block(i, _):
        here_rows = block_rows(i)
        dt = softplus(r.steps[here_rows])
        log = -dt * rates
        cum = exact_dot(ones, log)
        cum_across = exact_across(log, upper)
        dt_across = exact_across(dt, same)
        grown = jnp.exp(cum)
        for heads, dim, size, offset, key_at in groups:
            columns_here = pl.ds(offset, size)
            values = r.values[here_rows, columns_here]
            k = r.values[here_rows, pl.ds(key_at, state_len)]
            q = r.values[here_rows, pl.ds(key_at + 2 * state_len, state_len)]
            scores = lax.dot_general(q, k, (((1,), (1,)), ((), ())), preferred_element_type=F32)
            carried = jnp.dot(q, r.states[i, :, columns_here], preferred_element_type=F32)
            carried = carried * spread(grown, heads, dim)
            inside = []
            span = max(dim, LANES)
            per = span // dim
            for first in range(0, len(heads), per):
                part_values = values[:, first * dim : first * dim + span]
                part = None
                for j in range(per):
                    h = heads[first + j]
                    gap = cum[:, h : h + 1] - cum_across[h : h + 1]
                    decays = jnp.exp(jnp.where(causal, gap, FAR))
                    w = (scores * decays * dt_across[h : h + 1]).astype(BF16)
                    got = jnp.dot(w, part_values, preferred_element_type=F32)
                    part = got if part is None else jnp.where(lane >= j * dim, got, part)
                inside.append(part)
            r.inner[here_rows, columns_here] = jnp.concatenate(inside, axis=1) + carried
        return 0

    lax.fori_loop(0, blocks // 2, inside_block, 0)

    pair_copy.wait_recv()
    mine, mine_log = opened(r.packed)
    theirs, theirs_log = opened(r.beside)
    front = y == 0
    lead = jnp.where(front, mine, theirs)
    lead_log = jnp.where(front, mine_log, theirs_log)
    trail = jnp.where(front, theirs, mine)
    trail_log = jnp.where(front, theirs_log, mine_log)
    r.both[:state_len] = lead * jnp.exp(trail_log) + trail
    r.both[state_len:] = jnp.broadcast_to(lead_log + trail_log, (8, width))
    r.ahead[:state_len] = lead
    r.ahead[state_len:] = jnp.broadcast_to(lead_log, (8, width))
    r.state[...] = jnp.zeros_like(r.state)
    r.before_log[...] = jnp.zeros_like(r.before_log)
    hops = r.passed.shape[0]

    def line_copy(s):
        target = {OUTER: (z + (1 << s)) % count}
        return remote(r.passed.at[s], r.arrived.at[s], r.line_send.at[s], r.line_recv.at[s], target)

    for s in range(hops):

        @pl.when(z + (1 << s) < count)
        def _():
            pack(r.passed.at[s], r.both[:state_len], r.both[state_len : state_len + 1])
            line_copy(s).start()

        if s == 0:
            lax.fori_loop(blocks // 2, blocks, inside_block, 0)
        if s == hops - 1:
            start_line(z == 0, *rest)
            start_line(falling, *both_outward)

        @pl.when(z >= 1 << s)
        def _():
            line_copy(s).wait_recv()
            before, before_log = opened(r.arrived.at[s])
            r.state[...] = before * jnp.exp(r.before_log[0:1]) + r.state[...]
            r.before_log[...] = r.before_log[...] + before_log
            r.both[:state_len] = before * jnp.exp(r.both[state_len : state_len + 1]) + r.both[:state_len]
            r.both[state_len:] = r.both[state_len:] + before_log

    @pl.when(y == 1)
    def _():
        r.state[...] = r.state[...] * jnp.exp(r.ahead[state_len : state_len + 1]) + r.ahead[:state_len]

    r.entering[...] = r.state[...].astype(BF16)
    start_line(rising, (0, mate), (1, mate))
    for index in range(7, len(loads)):
        loads[index].wait()

    def near_mix(index):
        return remote(
            r.mix_core.at[index], r.mix_from.at[index], r.mix_send.at[index], r.mix_recv.at[index], near
        )

    across_mix = remote(r.mix_hop, r.mix_got, r.mix_send.at[2], r.mix_recv.at[2], across)

    per_share = share // BLOCK

    def project(b, _):
        which = b // per_share
        far, other = 1 - which // 2, 1 - which % 2
        source = flipped(x, far) * 2 + flipped(c, other)
        i = source * per_share + b % per_share
        here_rows = block_rows(i)
        grown = jnp.exp(r.logs[here_rows])
        result = None
        for heads, dim, size, offset, key_at in groups:
            columns_here = pl.ds(offset, size)
            q = r.values[here_rows, pl.ds(key_at + 2 * state_len, state_len)]
            carried = jnp.dot(q, r.entering[:, columns_here], preferred_element_type=F32)
            mixed = r.inner[here_rows, columns_here] + carried * spread(grown, heads, dim)
            gated = mixed * silu(r.gates[here_rows, columns_here].astype(F32))
            squares = gated * gated
            span = max(dim, LANES)
            per = span // dim
            normed = []
            for first in range(0, len(heads), per):
                at = first * dim
                part = squares[:, at : at + span]
                means = None
                for j in range(per):
                    if per == 1:
                        means = jnp.sum(part, axis=1, keepdims=True)
                    else:
                        ours = (lane >= j * dim) & (lane < (j + 1) * dim)
                        single = jnp.sum(jnp.where(ours, part, 0.0), axis=1, keepdims=True)
                        means = single if means is None else jnp.where(lane >= j * dim, single, means)
                normed.append(gated[:, at : at + span] * lax.rsqrt(means * (1.0 / dim) + EPS))
            normed = jnp.concatenate(normed, axis=1) * r.gain[:, columns_here]
            product = jnp.dot(normed.astype(BF16), r.out_rows[columns_here], preferred_element_type=F32)
            result = product if result is None else result + product
        part_rows = pl.ds(pl.multiple_of(b % per_share * BLOCK, BLOCK), BLOCK)

        @pl.when(other == 1)
        def _():
            r.mix_core[far, part_rows] = result.astype(BF16)

        @pl.when(other == 0)
        def _():
            r.mix_local[far, part_rows] = result

        @pl.when((other == 1) & (b % per_share == per_share - 1))
        def _():
            near_mix(far).start()

        @pl.when(b == 2 * per_share - 1)
        def _():
            near_mix(1).wait_recv()
            r.mix_hop[...] = (r.mix_local[1] + r.mix_from[1].astype(F32)).astype(BF16)
            across_mix.start()

        return 0

    lax.fori_loop(0, blocks, project, 0)
    pumps(0, 4)
    near_mix(0).wait_recv()
    across_mix.wait_recv()

    def place(core, d_one, d_two):
        return (flipped(pair, d_one) * 2 + flipped(x, d_two)) * 2 + core

    mine_at = place(c, 0, 0)
    tile = BLOCK // 2

    def norms(i, _):
        here = pl.ds(pl.multiple_of(i * tile, tile), tile)
        mix = r.mix_local[0, here] + r.mix_from[0, here].astype(F32) + r.mix_got[here].astype(F32)
        mixed = r.out[here].astype(F32) + unit_rms(mix) * r.gains[0:1]
        r.mixed[here] = mixed
        r.rows[mine_at, here] = (unit_rms(mixed) * r.gains[1:2]).astype(BF16)
        return 0

    lax.fori_loop(0, share // tile, norms, 0)

    def passing(slot, index, partner):
        return remote(r.rows.at[slot], r.rows.at[slot], r.rows_send.at[index], r.rows_recv.at[slot], partner)

    for index, partner in enumerate((upright, across, near)):
        passing(mine_at, index, partner).start()
    start_line(z == 0, *outward[1])
    pumps(4, 6)
    own_side(2).start()

    def complete(m):
        loads[4 + m].wait()
        for source in range(count):
            relay(m, source).wait_recv()

    def kept_at(core, j):
        return (1 - core) * j + core * (j % 2 * 2 + j // 2)

    complete(0)

    def open_gate(slot, at):
        gate = jnp.dot(r.rows[slot], r.gate_all[...], preferred_element_type=F32)
        r.hidden[at] = silu(gate).astype(BF16)

    def gates(j, _):
        d_one, d_two = j % 2, j // 2
        slot = place(c, d_one, d_two)

        @pl.when(j > 0)
        def _():
            passing(slot, 0, near).wait_recv()
            passing(slot, 3 + j, near).start()

        @pl.when(j == 1)
        def _():
            passing(slot, 3, across).start()
            to_line(2, mate).start()

            @pl.when(first_z > 0)
            def _():
                for m, target in outward[2]:
                    to_line(m, target).start()

        open_gate(slot, kept_at(c, j))
        slot = place(1 - c, d_one, d_two)
        passing(slot, 0, near).wait_recv()
        open_gate(slot, 4 + kept_at(1 - c, j))
        return 0

    lax.fori_loop(0, 3, gates, 0)
    complete(1)

    def expand(j, _):
        for core, first in ((c, 0), (1 - c, 4)):
            at = first + kept_at(core, j)
            up = jnp.dot(r.rows[place(core, j % 2, j // 2)], r.up_all[...], preferred_element_type=F32)
            hidden = r.hidden[at].astype(F32) * up
            column = lax.broadcasted_iota(jnp.int32, hidden.shape, 1)
            r.hidden[at] = jnp.where(column >= pair * overlap, hidden, 0.0).astype(BF16)
        return 0

    lax.fori_loop(0, 3, expand, 0)
    start_line(first_z == 0, *outward[2])
    pump(2, mate)
    lax.fori_loop(3, 4, gates, 0)
    lax.fori_loop(3, 4, expand, 0)

    chunk = r.got_one.shape[-1]
    per_chunk = chunk // rows
    chunks = features // chunk
    first_chunk = 2 * first_z * rows // chunk

    def chunk_at(k):
        return (first_chunk + k) % chunks

    def pump_chunk(k):
        for index in range(per_chunk):
            block = chunk_at(k) * per_chunk + index

            @pl.when((block % 2 == y) & (block // 2 // 2 != z // 2))
            def _():
                pump(2, block // 2)

    def near_copy(k):
        return remote(
            r.to_core.at[k % RING], r.from_core.at[k], r.core_send.at[k % RING], r.core_recv.at[k], near
        )

    def two_copy(k):
        return remote(r.hop_two.at[k % RING], r.got_two.at[k], r.two_send.at[k % RING], r.two_recv.at[k], two)

    def one_copy(k):
        return remote(r.hop_one.at[k % RING], r.got_one.at[k], r.one_send.at[k % RING], r.one_recv.at[k], one)

    def local_at(k, j):
        slot = k % RING
        start = pl.multiple_of((slot % 2 * 4 + j) * chunk, LANES)
        return slot // 2, slice(None), pl.ds(start, chunk)

    loads[6].wait()
    for k in range(AHEAD):
        pump_chunk(k)

    def reduce_step(k, _):
        @pl.when(k < chunks)
        def _():
            for index in range(per_chunk):
                block = chunk_at(k) * per_chunk + index

                @pl.when(block % 2 != y)
                def _():
                    relay(2, block // 2).wait_recv()

            @pl.when(k >= RING)
            def _():
                near_copy(k).wait_send()

            at = pl.ds(pl.multiple_of(chunk_at(k) * chunk, chunk), chunk)
            weights = r.down_all[at]
            for j in range(4):
                r.to_core[k % RING, j] = lax.dot_general(
                    r.hidden[4 + j], weights, (((1,), (1,)), ((), ())), preferred_element_type=F32
                ).astype(BF16)
            near_copy(k).start()
            for j in range(4):
                r.mix_local[local_at(k, j)] = lax.dot_general(
                    r.hidden[j], weights, (((1,), (1,)), ((), ())), preferred_element_type=F32
                )

        @pl.when((k >= 1) & (k < chunks + 1))
        def _():
            p = k - 1
            near_copy(p).wait_recv()

            @pl.when(p >= RING)
            def _():
                two_copy(p).wait_send()

            for index, j in enumerate((3, 2)):
                total = r.mix_local[local_at(p, j)] + r.from_core[p, j].astype(F32)
                r.hop_two[p % RING, index] = total.astype(BF16)
            two_copy(p).start()
            for j in range(2):
                r.mix_local[local_at(p, j)] = r.mix_local[local_at(p, j)] + r.from_core[p, j].astype(F32)

        @pl.when((k >= 2) & (k < chunks + 2))
        def _():
            p = k - 2
            two_copy(p).wait_recv()

            @pl.when(p >= RING)
            def _():
                one_copy(p).wait_send()

            total = r.mix_local[local_at(p, 1)] + r.got_two[p, 0].astype(F32)
            r.hop_one[p % RING] = total.astype(BF16)
            one_copy(p).start()

        @pl.when(k >= 3)
        def _():
            p = k - 3
            one_copy(p).wait_recv()
            total = r.mix_local[local_at(p, 0)] + r.got_two[p, 1].astype(F32) + r.got_one[p].astype(F32)
            r.ffn[:, pl.ds(pl.multiple_of(chunk_at(p) * chunk, chunk), chunk)] = total

        @pl.when(k < chunks - AHEAD)
        def _():
            pump_chunk(k + AHEAD)

        return 0

    lax.fori_loop(0, chunks + 3, reduce_step, 0)

    def finish(i, _):
        here = pl.ds(pl.multiple_of(i * tile, tile), tile)
        r.out[here] = (r.mixed[here] + 0.5 * unit_rms(r.ffn[here]) * r.gains[2:3]).astype(BF16)
        return 0

    lax.fori_loop(0, share // tile, finish, 0)

    @pl.when(~last)
    def _():
        for index in range(4):
            halo_copy(index, side).wait_send()

    pair_copy.wait_send()

    for s in range(hops):

        @pl.when(z + (1 << s) < count)
        def _():
            line_copy(s).wait_send()

    for m in range(3):
        for target in sources:
            to_line(m, target).wait_send()
        for source in range(count):
            relay(m, source).wait_send()
    near_mix(0).wait_send()
    near_mix(1).wait_send()
    across_mix.wait_send()
    for index in range(7):
        passing(mine_at, index, near).wait_send()
    for slot in range(min(RING, chunks)):
        near_copy(slot).wait_send()
        two_copy(slot).wait_send()
        one_copy(slot).wait_send()


def layer(
    residual,
    small_heads,
    large_heads,
    state_keys,
    state_queries,
    small_gate,
    large_gate,
    small_step,
    large_step,
    small_taps,
    large_taps,
    key_taps,
    query_taps,
    small_decay,
    large_decay,
    small_gain,
    large_gain,
    small_out,
    large_out,
    mixer_gain,
    ffn_in_gain,
    gate_proj,
    up_proj,
    down_proj,
    ffn_out_gain,
):
    length, features = residual.shape
    state_len = state_keys.shape[-1]
    key_rows = state_keys.reshape(length, -1)
    query_rows = state_queries.reshape(length, -1)
    heads_a = small_step.shape[1]
    heads_b = large_step.shape[1]
    heads = heads_a + heads_b
    width_a = small_heads.shape[1]
    width_b = large_heads.shape[1]
    width = width_a + width_b
    everything = width + key_rows.shape[1] + query_rows.shape[1]
    sizes = ((heads_a, width_a // heads_a), (heads_b, width_b // heads_b), state_len)
    steps = jnp.pad(
        jnp.concatenate([small_step, large_step], axis=1), ((0, 0), (0, SLOTS - heads))
    )
    taps_len = small_taps.shape[0]
    share = length // lax.axis_size(HEADS)
    rows, columns = down_proj.shape
    count = lax.axis_size(OUTER)
    wide = half_width(columns)
    chunk = max(rows, CHUNK)
    chunks = features // chunk
    blocks = length // BLOCK
    vmem = pl.BlockSpec(memory_space=pltpu.VMEM)
    hbm = pl.BlockSpec(memory_space=pl.ANY)
    smem = pl.BlockSpec(memory_space=pltpu.SMEM)
    dma = pltpu.SemaphoreType.DMA
    operands = {
        "small": (small_heads, hbm),
        "large": (large_heads, hbm),
        "keys": (key_rows, hbm),
        "queries": (query_rows, hbm),
        "small_gate": (small_gate, hbm),
        "large_gate": (large_gate, hbm),
        "small_out": (small_out, hbm),
        "large_out": (large_out, hbm),
        "residual": (residual, hbm),
        "gate_proj": (gate_proj, hbm),
        "up_proj": (up_proj, hbm),
        "down_proj": (down_proj, hbm),
        "steps": (steps, vmem),
        "small_decay": (small_decay, smem),
        "large_decay": (large_decay, smem),
        "small_taps": (small_taps, vmem),
        "large_taps": (large_taps, vmem),
        "key_taps": (key_taps, vmem),
        "query_taps": (query_taps, vmem),
        "small_gain": (small_gain, vmem),
        "large_gain": (large_gain, vmem),
        "mixer_gain": (mixer_gain, vmem),
        "ffn_in_gain": (ffn_in_gain, vmem),
        "ffn_out_gain": (ffn_out_gain, vmem),
    }
    packed = (state_len + TAIL, width)
    opened = (state_len + 8, width)
    hops = max(1, (count - 1).bit_length())
    scratch = {
        "values": pltpu.VMEM((length, everything), BF16),
        "gates": pltpu.VMEM((length, width), BF16),
        "out_rows": pltpu.VMEM((width, features), BF16),
        "gate_all": pltpu.VMEM((features, wide), BF16),
        "up_all": pltpu.VMEM((features, wide), BF16),
        "down_all": pltpu.VMEM((features, wide), BF16),
        "taps": pltpu.VMEM((taps_len, everything), F32),
        "gain": pltpu.VMEM((1, width), F32),
        "gains": pltpu.VMEM((3, features), F32),
        "halo": pltpu.VMEM((HALO, everything), BF16),
        "before": pltpu.VMEM((HALO, everything), BF16),
        "state": pltpu.VMEM((state_len, width), F32),
        "states": pltpu.VMEM((blocks, state_len, width), BF16),
        "total": pltpu.VMEM((1, SLOTS), F32),
        "logs": pltpu.VMEM((length, SLOTS), F32),
        "inner": pltpu.VMEM((length, width), F32),
        "packed": pltpu.VMEM(packed, BF16),
        "beside": pltpu.VMEM(packed, BF16),
        "passed": pltpu.VMEM((hops, *packed), BF16),
        "arrived": pltpu.VMEM((hops, *packed), BF16),
        "before_log": pltpu.VMEM((8, width), F32),
        "both": pltpu.VMEM(opened, F32),
        "ahead": pltpu.VMEM(opened, F32),
        "entering": pltpu.VMEM((state_len, width), BF16),
        "mix_core": pltpu.VMEM((2, share, features), BF16),
        "mix_from": pltpu.VMEM((2, share, features), BF16),
        "mix_local": pltpu.VMEM((2, share, features), F32),
        "mix_hop": pltpu.VMEM((share, features), BF16),
        "mix_got": pltpu.VMEM((share, features), BF16),
        "mixed": pltpu.VMEM((share, features), F32),
        "rows": pltpu.VMEM((8, share, features), BF16),
        "hidden": pltpu.VMEM((8, share, wide), BF16),
        "to_core": pltpu.VMEM((RING, 4, share, chunk), BF16),
        "from_core": pltpu.VMEM((chunks, 4, share, chunk), BF16),
        "hop_two": pltpu.VMEM((RING, 2, share, chunk), BF16),
        "got_two": pltpu.VMEM((chunks, 2, share, chunk), BF16),
        "hop_one": pltpu.VMEM((RING, share, chunk), BF16),
        "got_one": pltpu.VMEM((chunks, share, chunk), BF16),
        "ffn": pltpu.VMEM((share, features), F32),
        "halo_send": dma((4,)),
        "halo_recv": dma((4,)),
        "load_sem": dma((12,)),
        "send": dma((3, count)),
        "recv": dma((3, count)),
        "side_send": dma((3, count)),
        "side_recv": dma((3, count)),
        "state_send": dma((1,)),
        "state_recv": dma((1,)),
        "line_send": dma((hops,)),
        "line_recv": dma((hops,)),
        "mix_send": dma((3,)),
        "mix_recv": dma((3,)),
        "rows_send": dma((7,)),
        "rows_recv": dma((8,)),
        "core_send": dma((RING,)),
        "core_recv": dma((chunks,)),
        "two_send": dma((RING,)),
        "two_recv": dma((chunks,)),
        "one_send": dma((RING,)),
        "one_recv": dma((chunks,)),
    }
    names = (*operands, "out", *scratch)
    return pl.pallas_call(
        functools.partial(layer_kernel, names, sizes, 2 * wide - columns),
        in_specs=[spec for _, spec in operands.values()],
        out_specs=vmem,
        out_shape=jax.ShapeDtypeStruct((share, features), BF16),
        scratch_shapes=list(scratch.values()),
        compiler_params=pltpu.CompilerParams(
            collective_id=0, has_side_effects=True, vmem_limit_bytes=VMEM_BYTES
        ),
        cost_estimate=pl.CostEstimate(
            flops=40_000_000_000, bytes_accessed=share * features, transcendentals=0
        ),
        name="layer",
    )(*[array for array, _ in operands.values()])


def solution(mesh):
    placed = (
        P(SEQ, None),
        P(SEQ, HEADS),
        P(SEQ, HEADS),
        P(SEQ, HEADS, None),
        P(SEQ, HEADS, None),
        P(SEQ, HEADS),
        P(SEQ, HEADS),
        P(SEQ, HEADS),
        P(SEQ, HEADS),
        P(None, HEADS),
        P(None, HEADS),
        P(None, HEADS, None),
        P(None, HEADS, None),
        P(HEADS),
        P(HEADS),
        P(HEADS),
        P(HEADS),
        P(HEADS, None),
        P(HEADS, None),
        P(),
        P(),
        P(SEQ, HEADS),
        P(SEQ, HEADS),
        P(SEQ, HEADS),
        P(),
    )
    outer, heads = mesh.shape["sp"] // 2, mesh.shape["tp"] // 2
    cut = jax.sharding.Mesh(mesh.devices.reshape(outer, 2, heads, 2), (OUTER, INNER, CHIP, CORE))
    return jax.shard_map(layer, mesh=cut, in_specs=placed, out_specs=P((*SEQ, *HEADS), None), check_vma=False)
```

```python
import functools
import types

import jax
import jax.numpy as jnp
from jax import lax
from jax.experimental import pallas as pl
from jax.experimental.pallas import tpu as pltpu
from jax.sharding import PartitionSpec as P

BLOCK = 128
HALO = 16
LANES = 128
SLOTS = 8
TAIL = 16
CHUNK = 256
RING = 4
AHEAD = 4


EPS = 1e-06
OUTER, INNER = "so", "si"
SEQ = (OUTER, INNER)
CHIP, CORE = "tx", "tc"
HEADS = (CHIP, CORE)
MESH = pl.DeviceIdType.MESH
VMEM_BYTES = 64 * 1024 * 1024 - 128 * 1024
FAR = -1e30
F32 = jnp.float32
BF16 = jnp.bfloat16


def silu(x):
    return x / (1.0 + jnp.exp(-x))


def softplus(x):
    return jnp.maximum(x, 0.0) + jnp.log1p(jnp.exp(-jnp.abs(x)))


def exact_dot(a, b):
    return lax.dot_general(
        a, b, (((1,), (0,)), ((), ())), precision=lax.Precision.HIGHEST, preferred_element_type=F32
    )


def exact_across(a, b):
    return lax.dot_general(
        a, b, (((0,), (0,)), ((), ())), precision=lax.Precision.HIGHEST, preferred_element_type=F32
    )


def lower(n):
    rows = lax.broadcasted_iota(jnp.int32, (n, n), 0)
    return rows >= lax.broadcasted_iota(jnp.int32, (n, n), 1)


def spread(columns, heads, dim):
    rows = columns.shape[0]
    parts = []
    if dim >= LANES:
        for h in heads:
            parts.append(jnp.broadcast_to(columns[:, h : h + 1], (rows, dim)))
    else:
        per = LANES // dim
        lane = lax.broadcasted_iota(jnp.int32, (rows, LANES), 1)
        for first in range(0, len(heads), per):
            part = jnp.broadcast_to(columns[:, heads[first] : heads[first] + 1], (rows, LANES))
            for j in range(1, per):
                h = heads[first + j]
                part = jnp.where(lane >= j * dim, columns[:, h : h + 1], part)
            parts.append(part)
    return jnp.concatenate(parts, axis=1)


def unit_rms(values):
    return values * lax.rsqrt(jnp.mean(values * values, axis=-1, keepdims=True) + EPS)


def flipped(value, by):
    return value + by * (1 - 2 * value)


def half_width(columns):
    return (columns // LANES + 1) // 2 * LANES


def greet(partners):
    barrier = pltpu.get_barrier_semaphore()
    for partner in partners:
        pl.semaphore_signal(barrier, inc=1, device_id=partner, device_id_type=MESH)
    pl.semaphore_wait(barrier, len(partners))


def remote(source, target, send, recv, partner):
    copy = pltpu.make_async_remote_copy(
        src_ref=source,
        dst_ref=target,
        send_sem=send,
        recv_sem=recv,
        device_id=partner,
        device_id_type=MESH,
    )
    return copy


def layer_kernel(names, sizes, base, *refs):
    r = types.SimpleNamespace(**dict(zip(names, refs, strict=True)))
    (heads_a, dim_a), (heads_b, dim_b), state_len = sizes
    width_a, width_b = heads_a * dim_a, heads_b * dim_b
    width = width_a + width_b
    groups = (
        (list(range(heads_a)), dim_a, width_a, 0, width),
        (list(range(heads_a, heads_a + heads_b)), dim_b, width_b, width_a, width + state_len),
    )
    length, everything = r.values.shape
    blocks = length // BLOCK
    share, features = r.out.shape
    count = lax.axis_size(OUTER)
    z, y = lax.axis_index(OUTER), lax.axis_index(INNER)
    x, c = lax.axis_index(CHIP), lax.axis_index(CORE)
    pair = z % 2
    first_z = z - pair
    position = 2 * z + y
    side = {INNER: 1 - y}
    near = {CORE: 1 - c}
    across = {CHIP: 1 - x}
    upright = {OUTER: first_z + 1 - pair}
    one = {OUTER: z + (1 - c) * (1 - 2 * pair), CHIP: flipped(x, c)}
    two = {OUTER: z + c * (1 - 2 * pair), CHIP: flipped(x, 1 - c)}
    line = [{OUTER: (z + d) % count} for d in range(1, count)]
    turn = [{OUTER: (z + d) % count, INNER: 1 - y} for d in (1, count - 1)]
    greet([side, near, across, *line, *turn])

    inputs = (r.small, r.large, r.keys, r.queries)
    column = 0
    halo_columns = []
    for ref in inputs:
        halo_columns.append(pl.ds(column, ref.shape[1]))
        column += ref.shape[1]

    def halo_copy(index, partner):
        return remote(
            inputs[index].at[pl.ds(length - HALO, HALO)],
            r.halo.at[:, halo_columns[index]],
            r.halo_send.at[index],
            r.halo_recv.at[index],
            partner,
        )

    next_z = (z + 1) % count
    last = position == 2 * count - 1

    @pl.when(y == 0)
    def _():
        for index in range(4):
            halo_copy(index, side).start()

    @pl.when((y == 1) & ~last)
    def _():
        for index in range(4):
            halo_copy(index, {OUTER: next_z, INNER: 0}).start()

    loads = []

    def load(source, target):
        copy = pltpu.make_async_copy(source, target, r.load_sem.at[len(loads)])
        copy.start()
        loads.append(copy)

    for index, ref in enumerate(inputs):
        load(ref, r.values.at[:, halo_columns[index]])

    for index in range(4):
        loads[index].wait()

    @pl.when(position > 0)
    def _():
        for index in range(4):
            halo_copy(index, side).wait_recv()
        r.before[...] = r.halo[...]

    @pl.when(position == 0)
    def _():
        r.before[...] = jnp.zeros_like(r.before)

    shards = (r.gate_proj, r.up_proj, r.down_proj)
    gathered = (r.gate_all, r.up_all, r.down_all)
    rows, columns = r.gate_proj.shape
    wide = r.gate_all.shape[1]

    extra = wide - base

    def half(m, member, part):
        if part:
            return shards[m].at[:, pl.ds(base, extra)]
        return shards[m].at[:, pl.ds(pl.multiple_of(member * (columns - base), LANES), base)]

    def piece(m, source, part):
        here = pl.ds(pl.multiple_of((source * 2 + y) * rows, rows), rows)
        return gathered[m].at[here, pl.ds(base, extra) if part else pl.ds(0, base)]

    class Pieces:
        def __init__(self, make, member):
            self.make, self.member = make, member

        def each(self, act):
            act(self.make(0))
            if extra:

                @pl.when((self.member + c) % 2 == 0)
                def _():
                    act(self.make(1))

        def start(self):
            self.each(lambda copy: copy.start())

        def wait_send(self):
            self.each(lambda copy: copy.wait_send())

        def wait_recv(self):
            self.each(lambda copy: copy.wait_recv())

        def wait(self):
            self.each(lambda copy: copy.wait())

    def to_line(m, target):
        def make(p):
            return remote(
                half(m, target % 2, p),
                piece(m, z, p),
                r.send.at[p, m, target],
                r.recv.at[p, m, z],
                {OUTER: target},
            )

        return Pieces(make, target)

    def sideways(m, source, own, receiving):
        def make(p):
            there = piece(m, source, p)
            here = half(m, pair, p) if own else there
            sems = (r.send, r.recv) if receiving else (r.side_send, r.side_recv)
            return remote(here, there, sems[0].at[p, m, source], sems[1].at[p, m, source], side)

        return Pieces(make, z)

    def from_line(m, source):
        return sideways(m, source, False, True)

    def own_side(m):
        return sideways(m, z, True, False)

    def relay(m, source):
        return sideways(m, source, False, False)

    def own_load(m):
        return Pieces(
            lambda p: pltpu.make_async_copy(half(m, pair, p), piece(m, z, p), r.own_sem.at[p, m]), z
        )

    if extra:

        @pl.when((z + c) % 2 == 1)
        def _():
            for ref in gathered:
                ref[:, pl.ds(base, extra)] = jnp.zeros((features, extra), BF16)

    mate = first_z + 1 - pair
    lowest = (count - first_z) // count
    crossing = [lowest * (count + 1 - q) + (1 - lowest) * ((first_z + q) % count) for q in range(2, count)]
    sources = [*crossing[:1], mate, *crossing[1:]]

    def pump(m, source):
        from_line(m, source).wait_recv()
        relay(m, source).start()

    edge = (z == 0) | (z == count - 1)

    def pump(m, source):
        from_line(m, source).wait_recv()
        relay(m, source).start()

    def start_line(condition, *pieces):
        @pl.when(condition)
        def _():
            for m, target in pieces:
                to_line(m, target).start()

    outward = [[(m, target) for target in crossing] for m in range(3)]
    both_outward = [*outward[0], *outward[1]]
    rest = [*outward[0][1:], (0, mate), (1, mate)]
    early = [(1, mate), *outward[0][1:], outward[1][0]]
    rising = (pair == 0) & ~edge
    falling = (pair == 1) & ~edge
    start_line(edge, outward[0][0])
    start_line(z == 0, (0, mate))
    start_line(z == count - 1, *rest, *outward[1])
    start_line(falling, (0, mate), (1, mate))
    start_line(rising, *both_outward)
    queue = [(0, crossing[0]), (0, mate), (1, mate)]
    queue += [(0, source) for source in crossing[1:]] + [(1, source) for source in crossing]
    marks = [len(queue) * k // 6 for k in range(7)]

    def pumps(first, end):
        for m, source in queue[marks[first] : marks[end]]:
            pump(m, source)

    own_side(0).start()
    for m in range(3):
        own_load(m).start()
    load(r.small_gate, r.gates.at[:, pl.ds(0, width_a)])
    load(r.large_gate, r.gates.at[:, pl.ds(width_a, width_b)])
    load(r.small_out, r.out_rows.at[pl.ds(0, width_a)])
    load(r.large_out, r.out_rows.at[pl.ds(width_a, width_b)])
    me = x * 2 + c
    load(r.residual.at[pl.ds(pl.multiple_of(me * share, share), share)], r.out)

    r.taps[:, pl.ds(0, width_a)] = r.small_taps[...].astype(F32)
    r.taps[:, pl.ds(width_a, width_b)] = r.large_taps[...].astype(F32)
    column = width
    for ref in (r.key_taps, r.query_taps):
        for group in range(ref.shape[1]):
            for k in range(ref.shape[0]):
                r.taps[k : k + 1, pl.ds(column, state_len)] = ref[k, group : group + 1].astype(F32)
            column += state_len
    r.gain[0:1, pl.ds(0, width_a)] = r.small_gain[...].astype(F32)[None]
    r.gain[0:1, pl.ds(width_a, width_b)] = r.large_gain[...].astype(F32)[None]
    for index, ref in enumerate((r.mixer_gain, r.ffn_in_gain, r.ffn_out_gain)):
        r.gains[index : index + 1] = ref[...].astype(F32)[None]
    lanes = lax.broadcasted_iota(jnp.int32, (1, SLOTS), 1)
    decay = jnp.zeros((1, SLOTS), F32)
    for first, heads, ref in ((0, heads_a, r.small_decay), (heads_a, heads_b, r.large_decay)):
        for h in range(heads):
            decay = jnp.where(lanes == first + h, ref[h], decay)

    r.state[...] = jnp.zeros_like(r.state)
    r.total[...] = jnp.zeros_like(r.total)
    causal = lower(BLOCK)
    ones = causal.astype(F32)
    rates = jnp.exp(decay)

    def block_rows(i):
        return pl.ds(pl.multiple_of(i * BLOCK, BLOCK), BLOCK)

    def convolve(i, _):
        here_rows = block_rows(i)
        taps_len = r.taps.shape[0]
        for start in range(0, everything, LANES):
            here = pl.ds(start, LANES)
            now = r.values[here_rows, here]
            extended = jnp.concatenate([r.before[:, here], now], axis=0).astype(F32)
            summed = None
            for k in range(taps_len):
                first = HALO - taps_len + 1 + k
                term = r.taps[k : k + 1, here] * extended[first : first + BLOCK]
                summed = term if summed is None else summed + term
            r.before[:, here] = now[BLOCK - HALO :]
            r.values[here_rows, here] = silu(summed).astype(BF16)
        dt = softplus(r.steps[here_rows])
        cum = exact_dot(ones, -dt * rates)
        tail = cum[BLOCK - 1 : BLOCK]
        scale = dt * jnp.exp(tail - cum)
        kept = jnp.exp(tail)
        r.logs[here_rows] = r.total[...] + cum
        r.total[...] = r.total[...] + tail
        for heads, dim, size, offset, key_at in groups:
            columns_here = pl.ds(offset, size)
            values = r.values[here_rows, columns_here].astype(F32)
            u = (values * spread(scale, heads, dim)).astype(BF16)
            k = r.values[here_rows, pl.ds(key_at, state_len)]
            fresh = lax.dot_general(k, u, (((0,), (0,)), ((), ())), preferred_element_type=F32)
            old = r.state[:, columns_here]
            r.states[i, :, columns_here] = old.astype(BF16)
            r.state[:, columns_here] = old * spread(kept, heads, dim) + fresh
        return 0

    lax.fori_loop(0, blocks, convolve, 0)

    def pack(target, state, log):
        target[:state_len] = state.astype(BF16)
        high = log.astype(BF16)
        low = (log - high.astype(F32)).astype(BF16)
        row = lax.broadcasted_iota(jnp.int32, (TAIL, width), 0)
        both = jnp.where(row == 0, high.astype(F32), jnp.where(row == 1, low.astype(F32), 0.0))
        target[state_len:] = both.astype(BF16)

    def opened(ref):
        tail = ref[state_len:].astype(F32)
        return ref[:state_len].astype(F32), tail[0:1] + tail[1:2]

    pack(
        r.packed,
        r.state[...],
        jnp.concatenate([spread(r.total[...], heads, dim) for heads, dim, *_ in groups], axis=1),
    )
    pair_copy = remote(r.packed, r.beside, r.state_send.at[0], r.state_recv.at[0], side)
    pair_copy.start()
    own_side(1).start()
    own_side(2).start()

    upper = (
        lax.broadcasted_iota(jnp.int32, (BLOCK, BLOCK), 0)
        <= lax.broadcasted_iota(jnp.int32, (BLOCK, BLOCK), 1)
    ).astype(F32)
    same = (
        lax.broadcasted_iota(jnp.int32, (BLOCK, BLOCK), 0)
        == lax.broadcasted_iota(jnp.int32, (BLOCK, BLOCK), 1)
    ).astype(F32)
    lane = lax.broadcasted_iota(jnp.int32, (BLOCK, LANES), 1)

    def inside_block(i, _):
        here_rows = block_rows(i)
        dt = softplus(r.steps[here_rows])
        log = -dt * rates
        cum = exact_dot(ones, log)
        cum_across = exact_across(log, upper)
        dt_across = exact_across(dt, same)
        grown = jnp.exp(cum)
        for heads, dim, size, offset, key_at in groups:
            columns_here = pl.ds(offset, size)
            values = r.values[here_rows, columns_here]
            k = r.values[here_rows, pl.ds(key_at, state_len)]
            q = r.values[here_rows, pl.ds(key_at + 2 * state_len, state_len)]
            scores = lax.dot_general(q, k, (((1,), (1,)), ((), ())), preferred_element_type=F32)
            carried = jnp.dot(q, r.states[i, :, columns_here], preferred_element_type=F32)
            carried = carried * spread(grown, heads, dim)
            inside = []
            span = max(dim, LANES)
            per = span // dim
            for first in range(0, len(heads), per):
                part_values = values[:, first * dim : first * dim + span]
                part = None
                for j in range(per):
                    h = heads[first + j]
                    gap = cum[:, h : h + 1] - cum_across[h : h + 1]
                    decays = jnp.exp(jnp.where(causal, gap, FAR))
                    w = (scores * decays * dt_across[h : h + 1]).astype(BF16)
                    got = jnp.dot(w, part_values, preferred_element_type=F32)
                    part = got if part is None else jnp.where(lane >= j * dim, got, part)
                inside.append(part)
            r.inner[here_rows, columns_here] = jnp.concatenate(inside, axis=1) + carried
        return 0

    lax.fori_loop(0, blocks // 2, inside_block, 0)

    pair_copy.wait_recv()
    mine, mine_log = opened(r.packed)
    theirs, theirs_log = opened(r.beside)
    front = y == 0
    lead = jnp.where(front, mine, theirs)
    lead_log = jnp.where(front, mine_log, theirs_log)
    trail = jnp.where(front, theirs, mine)
    trail_log = jnp.where(front, theirs_log, mine_log)
    r.both[:state_len] = lead * jnp.exp(trail_log) + trail
    r.both[state_len:] = jnp.broadcast_to(lead_log + trail_log, (8, width))
    r.ahead[:state_len] = lead
    r.ahead[state_len:] = jnp.broadcast_to(lead_log, (8, width))
    r.state[...] = jnp.zeros_like(r.state)
    r.before_log[...] = jnp.zeros_like(r.before_log)
    hops = r.passed.shape[0]

    def line_copy(s):
        target = {OUTER: (z + (1 << s)) % count}
        return remote(r.passed.at[s], r.arrived.at[s], r.line_send.at[s], r.line_recv.at[s], target)

    for s in range(hops):

        @pl.when(z + (1 << s) < count)
        def _():
            pack(r.passed.at[s], r.both[:state_len], r.both[state_len : state_len + 1])
            line_copy(s).start()

        if s == 0:
            lax.fori_loop(blocks // 2, blocks, inside_block, 0)
        if s == hops - 1:
            start_line(z == 0, *early)
            start_line(falling, *both_outward)

        @pl.when(z >= 1 << s)
        def _():
            line_copy(s).wait_recv()
            before, before_log = opened(r.arrived.at[s])
            r.state[...] = before * jnp.exp(r.before_log[0:1]) + r.state[...]
            r.before_log[...] = r.before_log[...] + before_log
            r.both[:state_len] = before * jnp.exp(r.both[state_len : state_len + 1]) + r.both[:state_len]
            r.both[state_len:] = r.both[state_len:] + before_log

    @pl.when(y == 1)
    def _():
        r.state[...] = r.state[...] * jnp.exp(r.ahead[state_len : state_len + 1]) + r.ahead[:state_len]

    r.entering[...] = r.state[...].astype(BF16)
    start_line(rising, (0, mate), (1, mate))
    for index in range(4, len(loads)):
        loads[index].wait()

    def near_mix(index):
        return remote(
            r.mix_core.at[index], r.mix_from.at[index], r.mix_send.at[index], r.mix_recv.at[index], near
        )

    across_mix = remote(r.mix_hop, r.mix_got, r.mix_send.at[2], r.mix_recv.at[2], across)

    per_share = share // BLOCK

    def project(b, _):
        which = b // per_share
        far, other = 1 - which // 2, 1 - which % 2
        source = flipped(x, far) * 2 + flipped(c, other)
        i = source * per_share + b % per_share
        here_rows = block_rows(i)
        grown = jnp.exp(r.logs[here_rows])
        result = None
        for heads, dim, size, offset, key_at in groups:
            columns_here = pl.ds(offset, size)
            q = r.values[here_rows, pl.ds(key_at + 2 * state_len, state_len)]
            carried = jnp.dot(q, r.entering[:, columns_here], preferred_element_type=F32)
            mixed = r.inner[here_rows, columns_here] + carried * spread(grown, heads, dim)
            gated = mixed * silu(r.gates[here_rows, columns_here].astype(F32))
            squares = gated * gated
            span = max(dim, LANES)
            per = span // dim
            normed = []
            for first in range(0, len(heads), per):
                at = first * dim
                part = squares[:, at : at + span]
                means = None
                for j in range(per):
                    if per == 1:
                        means = jnp.sum(part, axis=1, keepdims=True)
                    else:
                        ours = (lane >= j * dim) & (lane < (j + 1) * dim)
                        single = jnp.sum(jnp.where(ours, part, 0.0), axis=1, keepdims=True)
                        means = single if means is None else jnp.where(lane >= j * dim, single, means)
                normed.append(gated[:, at : at + span] * lax.rsqrt(means * (1.0 / dim) + EPS))
            normed = jnp.concatenate(normed, axis=1) * r.gain[:, columns_here]
            product = jnp.dot(normed.astype(BF16), r.out_rows[columns_here], preferred_element_type=F32)
            result = product if result is None else result + product
        part_rows = pl.ds(pl.multiple_of(b % per_share * BLOCK, BLOCK), BLOCK)

        @pl.when(other == 1)
        def _():
            r.mix_core[far, part_rows] = result.astype(BF16)

        @pl.when(other == 0)
        def _():
            r.mix_local[far, part_rows] = result

        @pl.when((other == 1) & (b % per_share == per_share - 1))
        def _():
            near_mix(far).start()

        @pl.when(b == 2 * per_share - 1)
        def _():
            near_mix(1).wait_recv()
            r.mix_hop[...] = (r.mix_local[1] + r.mix_from[1].astype(F32)).astype(BF16)
            across_mix.start()

        return 0

    lax.fori_loop(0, blocks, project, 0)
    pumps(0, 4)
    near_mix(0).wait_recv()
    across_mix.wait_recv()

    def place(core, d_one, d_two):
        return (flipped(pair, d_one) * 2 + flipped(x, d_two)) * 2 + core

    mine_at = place(c, 0, 0)
    tile = BLOCK // 2

    def norms(i, _):
        here = pl.ds(pl.multiple_of(i * tile, tile), tile)
        mix = r.mix_local[0, here] + r.mix_from[0, here].astype(F32) + r.mix_got[here].astype(F32)
        mixed = r.out[here].astype(F32) + unit_rms(mix) * r.gains[0:1]
        r.mixed[here] = mixed
        r.rows[mine_at, here] = (unit_rms(mixed) * r.gains[1:2]).astype(BF16)
        return 0

    lax.fori_loop(0, share // tile, norms, 0)

    def passing(slot, index, partner):
        return remote(r.rows.at[slot], r.rows.at[slot], r.rows_send.at[index], r.rows_recv.at[slot], partner)

    for index, partner in enumerate((upright, across, near)):
        passing(mine_at, index, partner).start()
    start_line(z == 0, *outward[1][1:])
    to_line(2, mate).start()
    for m, target in outward[2][1:]:
        to_line(m, target).start()
    pumps(4, 6)

    def complete(m):
        own_load(m).wait()
        for source in range(count):
            relay(m, source).wait_recv()

    def kept_at(core, j):
        return (1 - core) * j + core * (j % 2 * 2 + j // 2)

    complete(0)

    def open_gate(slot, at):
        gate = jnp.dot(r.rows[slot], r.gate_all[...], preferred_element_type=F32)
        r.hidden[at] = silu(gate).astype(BF16)

    def gates(j, _):
        d_one, d_two = j % 2, j // 2
        slot = place(c, d_one, d_two)

        @pl.when(j > 0)
        def _():
            passing(slot, 0, near).wait_recv()
            passing(slot, 3 + j, near).start()

        @pl.when(j == 1)
        def _():
            passing(slot, 3, across).start()
            start_line(first_z > 0, outward[2][0])

        open_gate(slot, kept_at(c, j))
        slot = place(1 - c, d_one, d_two)
        passing(slot, 0, near).wait_recv()
        open_gate(slot, 4 + kept_at(1 - c, j))
        return 0

    lax.fori_loop(0, 3, gates, 0)
    complete(1)

    def expand(j, _):
        for core, first in ((c, 0), (1 - c, 4)):
            at = first + kept_at(core, j)
            up = jnp.dot(r.rows[place(core, j % 2, j // 2)], r.up_all[...], preferred_element_type=F32)
            hidden = r.hidden[at].astype(F32) * up
            column = lax.broadcasted_iota(jnp.int32, hidden.shape, 1)
            held = wide - (z + c) % 2 * extra
            r.hidden[at] = jnp.where(column < held, hidden, 0.0).astype(BF16)
        return 0

    lax.fori_loop(0, 3, expand, 0)
    start_line(first_z == 0, outward[2][0])
    pump(2, mate)
    lax.fori_loop(3, 4, gates, 0)
    lax.fori_loop(3, 4, expand, 0)

    chunk = r.got_one.shape[-1]
    per_chunk = chunk // rows
    chunks = features // chunk
    first_chunk = 2 * first_z * rows // chunk

    def chunk_at(k):
        return (first_chunk + k) % chunks

    def pump_chunk(k):
        for index in range(per_chunk):
            block = chunk_at(k) * per_chunk + index

            @pl.when((block % 2 == y) & (block // 2 // 2 != z // 2))
            def _():
                pump(2, block // 2)

    def near_copy(k):
        return remote(
            r.to_core.at[k % RING], r.from_core.at[k], r.core_send.at[k % RING], r.core_recv.at[k], near
        )

    def two_copy(k):
        return remote(r.hop_two.at[k % RING], r.got_two.at[k], r.two_send.at[k % RING], r.two_recv.at[k], two)

    def one_copy(k):
        return remote(r.hop_one.at[k % RING], r.got_one.at[k], r.one_send.at[k % RING], r.one_recv.at[k], one)

    def local_at(k, j):
        slot = k % RING
        start = pl.multiple_of((slot % 2 * 4 + j) * chunk, LANES)
        return slot // 2, slice(None), pl.ds(start, chunk)

    own_load(2).wait()
    for k in range(AHEAD):
        pump_chunk(k)

    def reduce_step(k, _):
        @pl.when(k < chunks)
        def _():
            for index in range(per_chunk):
                block = chunk_at(k) * per_chunk + index

                @pl.when(block % 2 != y)
                def _():
                    relay(2, block // 2).wait_recv()

            @pl.when(k >= RING)
            def _():
                near_copy(k).wait_send()

            at = pl.ds(pl.multiple_of(chunk_at(k) * chunk, chunk), chunk)
            weights = r.down_all[at]
            for j in range(4):
                r.to_core[k % RING, j] = lax.dot_general(
                    r.hidden[4 + j], weights, (((1,), (1,)), ((), ())), preferred_element_type=F32
                ).astype(BF16)
            near_copy(k).start()
            for j in range(4):
                r.mix_local[local_at(k, j)] = lax.dot_general(
                    r.hidden[j], weights, (((1,), (1,)), ((), ())), preferred_element_type=F32
                )

        @pl.when((k >= 1) & (k < chunks + 1))
        def _():
            p = k - 1
            near_copy(p).wait_recv()

            @pl.when(p >= RING)
            def _():
                two_copy(p).wait_send()

            for index, j in enumerate((3, 2)):
                total = r.mix_local[local_at(p, j)] + r.from_core[p, j].astype(F32)
                r.hop_two[p % RING, index] = total.astype(BF16)
            two_copy(p).start()
            for j in range(2):
                r.mix_local[local_at(p, j)] = r.mix_local[local_at(p, j)] + r.from_core[p, j].astype(F32)

        @pl.when((k >= 2) & (k < chunks + 2))
        def _():
            p = k - 2
            two_copy(p).wait_recv()

            @pl.when(p >= RING)
            def _():
                one_copy(p).wait_send()

            total = r.mix_local[local_at(p, 1)] + r.got_two[p, 0].astype(F32)
            r.hop_one[p % RING] = total.astype(BF16)
            one_copy(p).start()

        @pl.when(k >= 3)
        def _():
            p = k - 3
            one_copy(p).wait_recv()
            total = r.mix_local[local_at(p, 0)] + r.got_two[p, 1].astype(F32) + r.got_one[p].astype(F32)
            r.ffn[:, pl.ds(pl.multiple_of(chunk_at(p) * chunk, chunk), chunk)] = total

        @pl.when(k < chunks - AHEAD)
        def _():
            pump_chunk(k + AHEAD)

        return 0

    lax.fori_loop(0, chunks + 3, reduce_step, 0)

    def finish(i, _):
        here = pl.ds(pl.multiple_of(i * tile, tile), tile)
        r.out[here] = (r.mixed[here] + 0.5 * unit_rms(r.ffn[here]) * r.gains[2:3]).astype(BF16)
        return 0

    lax.fori_loop(0, share // tile, finish, 0)

    @pl.when(~last)
    def _():
        for index in range(4):
            halo_copy(index, side).wait_send()

    pair_copy.wait_send()

    for s in range(hops):

        @pl.when(z + (1 << s) < count)
        def _():
            line_copy(s).wait_send()

    for m in range(3):
        for target in sources:
            to_line(m, target).wait_send()
        for source in range(count):
            relay(m, source).wait_send()
    near_mix(0).wait_send()
    near_mix(1).wait_send()
    across_mix.wait_send()
    for index in range(7):
        passing(mine_at, index, near).wait_send()
    for slot in range(min(RING, chunks)):
        near_copy(slot).wait_send()
        two_copy(slot).wait_send()
        one_copy(slot).wait_send()


def layer(
    residual,
    small_heads,
    large_heads,
    state_keys,
    state_queries,
    small_gate,
    large_gate,
    small_step,
    large_step,
    small_taps,
    large_taps,
    key_taps,
    query_taps,
    small_decay,
    large_decay,
    small_gain,
    large_gain,
    small_out,
    large_out,
    mixer_gain,
    ffn_in_gain,
    gate_proj,
    up_proj,
    down_proj,
    ffn_out_gain,
):
    length, features = residual.shape
    state_len = state_keys.shape[-1]
    key_rows = state_keys.reshape(length, -1)
    query_rows = state_queries.reshape(length, -1)
    heads_a = small_step.shape[1]
    heads_b = large_step.shape[1]
    heads = heads_a + heads_b
    width_a = small_heads.shape[1]
    width_b = large_heads.shape[1]
    width = width_a + width_b
    everything = width + key_rows.shape[1] + query_rows.shape[1]
    sizes = ((heads_a, width_a // heads_a), (heads_b, width_b // heads_b), state_len)
    steps = jnp.pad(
        jnp.concatenate([small_step, large_step], axis=1), ((0, 0), (0, SLOTS - heads))
    )
    taps_len = small_taps.shape[0]
    share = length // lax.axis_size(HEADS)
    rows, columns = down_proj.shape
    count = lax.axis_size(OUTER)
    wide = half_width(columns)
    chunk = max(rows, CHUNK)
    chunks = features // chunk
    blocks = length // BLOCK
    vmem = pl.BlockSpec(memory_space=pltpu.VMEM)
    hbm = pl.BlockSpec(memory_space=pl.ANY)
    smem = pl.BlockSpec(memory_space=pltpu.SMEM)
    dma = pltpu.SemaphoreType.DMA
    operands = {
        "small": (small_heads, hbm),
        "large": (large_heads, hbm),
        "keys": (key_rows, hbm),
        "queries": (query_rows, hbm),
        "small_gate": (small_gate, hbm),
        "large_gate": (large_gate, hbm),
        "small_out": (small_out, hbm),
        "large_out": (large_out, hbm),
        "residual": (residual, hbm),
        "gate_proj": (gate_proj, hbm),
        "up_proj": (up_proj, hbm),
        "down_proj": (down_proj, hbm),
        "steps": (steps, vmem),
        "small_decay": (small_decay, smem),
        "large_decay": (large_decay, smem),
        "small_taps": (small_taps, vmem),
        "large_taps": (large_taps, vmem),
        "key_taps": (key_taps, vmem),
        "query_taps": (query_taps, vmem),
        "small_gain": (small_gain, vmem),
        "large_gain": (large_gain, vmem),
        "mixer_gain": (mixer_gain, vmem),
        "ffn_in_gain": (ffn_in_gain, vmem),
        "ffn_out_gain": (ffn_out_gain, vmem),
    }
    packed = (state_len + TAIL, width)
    opened = (state_len + 8, width)
    hops = max(1, (count - 1).bit_length())
    scratch = {
        "values": pltpu.VMEM((length, everything), BF16),
        "gates": pltpu.VMEM((length, width), BF16),
        "out_rows": pltpu.VMEM((width, features), BF16),
        "gate_all": pltpu.VMEM((features, wide), BF16),
        "up_all": pltpu.VMEM((features, wide), BF16),
        "down_all": pltpu.VMEM((features, wide), BF16),
        "taps": pltpu.VMEM((taps_len, everything), F32),
        "gain": pltpu.VMEM((1, width), F32),
        "gains": pltpu.VMEM((3, features), F32),
        "halo": pltpu.VMEM((HALO, everything), BF16),
        "before": pltpu.VMEM((HALO, everything), BF16),
        "state": pltpu.VMEM((state_len, width), F32),
        "states": pltpu.VMEM((blocks, state_len, width), BF16),
        "total": pltpu.VMEM((1, SLOTS), F32),
        "logs": pltpu.VMEM((length, SLOTS), F32),
        "inner": pltpu.VMEM((length, width), F32),
        "packed": pltpu.VMEM(packed, BF16),
        "beside": pltpu.VMEM(packed, BF16),
        "passed": pltpu.VMEM((hops, *packed), BF16),
        "arrived": pltpu.VMEM((hops, *packed), BF16),
        "before_log": pltpu.VMEM((8, width), F32),
        "both": pltpu.VMEM(opened, F32),
        "ahead": pltpu.VMEM(opened, F32),
        "entering": pltpu.VMEM((state_len, width), BF16),
        "mix_core": pltpu.VMEM((2, share, features), BF16),
        "mix_from": pltpu.VMEM((2, share, features), BF16),
        "mix_local": pltpu.VMEM((2, share, features), F32),
        "mix_hop": pltpu.VMEM((share, features), BF16),
        "mix_got": pltpu.VMEM((share, features), BF16),
        "mixed": pltpu.VMEM((share, features), F32),
        "rows": pltpu.VMEM((8, share, features), BF16),
        "hidden": pltpu.VMEM((8, share, wide), BF16),
        "to_core": pltpu.VMEM((RING, 4, share, chunk), BF16),
        "from_core": pltpu.VMEM((chunks, 4, share, chunk), BF16),
        "hop_two": pltpu.VMEM((RING, 2, share, chunk), BF16),
        "got_two": pltpu.VMEM((chunks, 2, share, chunk), BF16),
        "hop_one": pltpu.VMEM((RING, share, chunk), BF16),
        "got_one": pltpu.VMEM((chunks, share, chunk), BF16),
        "ffn": pltpu.VMEM((share, features), F32),
        "halo_send": dma((4,)),
        "halo_recv": dma((4,)),
        "load_sem": dma((9,)),
        "own_sem": dma((2, 3)),
        "send": dma((2, 3, count)),
        "recv": dma((2, 3, count)),
        "side_send": dma((2, 3, count)),
        "side_recv": dma((2, 3, count)),
        "state_send": dma((1,)),
        "state_recv": dma((1,)),
        "line_send": dma((hops,)),
        "line_recv": dma((hops,)),
        "mix_send": dma((3,)),
        "mix_recv": dma((3,)),
        "rows_send": dma((7,)),
        "rows_recv": dma((8,)),
        "core_send": dma((RING,)),
        "core_recv": dma((chunks,)),
        "two_send": dma((RING,)),
        "two_recv": dma((chunks,)),
        "one_send": dma((RING,)),
        "one_recv": dma((chunks,)),
    }
    names = (*operands, "out", *scratch)
    return pl.pallas_call(
        functools.partial(layer_kernel, names, sizes, columns - wide),
        in_specs=[spec for _, spec in operands.values()],
        out_specs=vmem,
        out_shape=jax.ShapeDtypeStruct((share, features), BF16),
        scratch_shapes=list(scratch.values()),
        compiler_params=pltpu.CompilerParams(
            collective_id=0, has_side_effects=True, vmem_limit_bytes=VMEM_BYTES
        ),
        cost_estimate=pl.CostEstimate(
            flops=40_000_000_000, bytes_accessed=share * features, transcendentals=0
        ),
        name="layer",
    )(*[array for array, _ in operands.values()])


def solution(mesh):
    placed = (
        P(SEQ, None),
        P(SEQ, HEADS),
        P(SEQ, HEADS),
        P(SEQ, HEADS, None),
        P(SEQ, HEADS, None),
        P(SEQ, HEADS),
        P(SEQ, HEADS),
        P(SEQ, HEADS),
        P(SEQ, HEADS),
        P(None, HEADS),
        P(None, HEADS),
        P(None, HEADS, None),
        P(None, HEADS, None),
        P(HEADS),
        P(HEADS),
        P(HEADS),
        P(HEADS),
        P(HEADS, None),
        P(HEADS, None),
        P(),
        P(),
        P(SEQ, HEADS),
        P(SEQ, HEADS),
        P(SEQ, HEADS),
        P(),
    )
    outer, heads = mesh.shape["sp"] // 2, mesh.shape["tp"] // 2
    cut = jax.sharding.Mesh(mesh.devices.reshape(outer, 2, heads, 2), (OUTER, INNER, CHIP, CORE))
    return jax.shard_map(
        layer, mesh=cut, in_specs=placed, out_specs=P((*SEQ, *HEADS), None), check_vma=False
    )
```

```python
import functools
import types

import jax
import jax.numpy as jnp
from jax import lax
from jax.experimental import pallas as pl
from jax.experimental.pallas import tpu as pltpu
from jax.sharding import PartitionSpec as P

BLOCK = 128
HALO = 16
LANES = 128
SLOTS = 8
TAIL = 16
CHUNK = 256
RING = 4
AHEAD = 4


EPS = 1e-06
OUTER, INNER = "so", "si"
SEQ = (OUTER, INNER)
CHIP, CORE = "tx", "tc"
HEADS = (CHIP, CORE)
MESH = pl.DeviceIdType.MESH
VMEM_BYTES = 64 * 1024 * 1024 - 128 * 1024
FAR = -1e30
F32 = jnp.float32
BF16 = jnp.bfloat16


def silu(x):
    half = 0.5 * x
    return half + half * jnp.tanh(half)


def softplus(x):
    return jnp.maximum(x, 0.0) + jnp.log1p(jnp.exp(-jnp.abs(x)))


def exact_dot(a, b):
    return lax.dot_general(
        a, b, (((1,), (0,)), ((), ())), precision=lax.Precision.HIGHEST, preferred_element_type=F32
    )


def exact_across(a, b):
    return lax.dot_general(
        a, b, (((0,), (0,)), ((), ())), precision=lax.Precision.HIGHEST, preferred_element_type=F32
    )


def lower(n):
    rows = lax.broadcasted_iota(jnp.int32, (n, n), 0)
    return rows >= lax.broadcasted_iota(jnp.int32, (n, n), 1)


def spread(columns, heads, dim):
    rows = columns.shape[0]
    parts = []
    if dim >= LANES:
        for h in heads:
            parts.append(jnp.broadcast_to(columns[:, h : h + 1], (rows, dim)))
    else:
        per = LANES // dim
        lane = lax.broadcasted_iota(jnp.int32, (rows, LANES), 1)
        for first in range(0, len(heads), per):
            part = jnp.broadcast_to(columns[:, heads[first] : heads[first] + 1], (rows, LANES))
            for j in range(1, per):
                h = heads[first + j]
                part = jnp.where(lane >= j * dim, columns[:, h : h + 1], part)
            parts.append(part)
    return jnp.concatenate(parts, axis=1)


def unit_rms(values):
    return values * lax.rsqrt(jnp.mean(values * values, axis=-1, keepdims=True) + EPS)


def flipped(value, by):
    return value + by * (1 - 2 * value)


def half_width(columns):
    return (columns // LANES + 1) // 2 * LANES


def greet(partners):
    barrier = pltpu.get_barrier_semaphore()
    for partner in partners:
        pl.semaphore_signal(barrier, inc=1, device_id=partner, device_id_type=MESH)
    pl.semaphore_wait(barrier, len(partners))


def remote(source, target, send, recv, partner):
    copy = pltpu.make_async_remote_copy(
        src_ref=source,
        dst_ref=target,
        send_sem=send,
        recv_sem=recv,
        device_id=partner,
        device_id_type=MESH,
    )
    return copy


def layer_kernel(names, sizes, base, *refs):
    r = types.SimpleNamespace(**dict(zip(names, refs, strict=True)))
    (heads_a, dim_a), (heads_b, dim_b), state_len = sizes
    width_a, width_b = heads_a * dim_a, heads_b * dim_b
    width = width_a + width_b
    groups = (
        (list(range(heads_a)), dim_a, width_a, 0, width),
        (list(range(heads_a, heads_a + heads_b)), dim_b, width_b, width_a, width + state_len),
    )
    length, everything = r.values.shape
    blocks = length // BLOCK
    share, features = r.out.shape
    count = lax.axis_size(OUTER)
    z, y = lax.axis_index(OUTER), lax.axis_index(INNER)
    x, c = lax.axis_index(CHIP), lax.axis_index(CORE)
    pair = z % 2
    first_z = z - pair
    position = 2 * z + y
    side = {INNER: 1 - y}
    near = {CORE: 1 - c}
    across = {CHIP: 1 - x}
    upright = {OUTER: first_z + 1 - pair}
    one = {OUTER: z + (1 - c) * (1 - 2 * pair), CHIP: flipped(x, c)}
    two = {OUTER: z + c * (1 - 2 * pair), CHIP: flipped(x, 1 - c)}
    line = [{OUTER: (z + d) % count} for d in range(1, count)]
    turn = [{OUTER: (z + d) % count, INNER: 1 - y} for d in (1, count - 1)]
    greet([side, near, across, *line, *turn])

    inputs = (r.small, r.large, r.keys, r.queries)
    column = 0
    halo_columns = []
    for ref in inputs:
        halo_columns.append(pl.ds(column, ref.shape[1]))
        column += ref.shape[1]

    def halo_copy(index, partner):
        return remote(
            inputs[index].at[pl.ds(length - HALO, HALO)],
            r.halo.at[:, halo_columns[index]],
            r.halo_send.at[index],
            r.halo_recv.at[index],
            partner,
        )

    next_z = (z + 1) % count
    last = position == 2 * count - 1

    @pl.when(y == 0)
    def _():
        for index in range(4):
            halo_copy(index, side).start()

    @pl.when((y == 1) & ~last)
    def _():
        for index in range(4):
            halo_copy(index, {OUTER: next_z, INNER: 0}).start()

    loads = []

    def load(source, target):
        copy = pltpu.make_async_copy(source, target, r.load_sem.at[len(loads)])
        copy.start()
        loads.append(copy)

    for index, ref in enumerate(inputs):
        load(ref, r.values.at[:, halo_columns[index]])

    for index in range(4):
        loads[index].wait()

    @pl.when(position > 0)
    def _():
        for index in range(4):
            halo_copy(index, side).wait_recv()
        r.before[...] = r.halo[...]

    @pl.when(position == 0)
    def _():
        r.before[...] = jnp.zeros_like(r.before)

    shards = (r.gate_proj, r.up_proj, r.down_proj)
    gathered = (r.gate_all, r.up_all, r.down_all)
    rows, columns = r.gate_proj.shape
    wide = r.gate_all.shape[1]

    extra = wide - base

    def half(m, member, part):
        if part:
            return shards[m].at[:, pl.ds(base, extra)]
        return shards[m].at[:, pl.ds(pl.multiple_of(member * (columns - base), LANES), base)]

    def piece(m, source, part):
        here = pl.ds(pl.multiple_of((source * 2 + y) * rows, rows), rows)
        return gathered[m].at[here, pl.ds(base, extra) if part else pl.ds(0, base)]

    class Pieces:
        def __init__(self, make, member):
            self.make, self.member = make, member

        def each(self, act):
            act(self.make(0))
            if extra:

                @pl.when((self.member + c) % 2 == 0)
                def _():
                    act(self.make(1))

        def start(self):
            self.each(lambda copy: copy.start())

        def wait_send(self):
            self.each(lambda copy: copy.wait_send())

        def wait_recv(self):
            self.each(lambda copy: copy.wait_recv())

        def wait(self):
            self.each(lambda copy: copy.wait())

    def to_line(m, target):
        def make(p):
            return remote(
                half(m, target % 2, p),
                piece(m, z, p),
                r.send.at[p, m, target],
                r.recv.at[p, m, z],
                {OUTER: target},
            )

        return Pieces(make, target)

    def sideways(m, source, own, receiving):
        def make(p):
            there = piece(m, source, p)
            here = half(m, pair, p) if own else there
            sems = (r.send, r.recv) if receiving else (r.side_send, r.side_recv)
            return remote(here, there, sems[0].at[p, m, source], sems[1].at[p, m, source], side)

        return Pieces(make, z)

    def from_line(m, source):
        return sideways(m, source, False, True)

    def own_side(m):
        return sideways(m, z, True, False)

    def relay(m, source):
        return sideways(m, source, False, False)

    def own_load(m):
        return Pieces(
            lambda p: pltpu.make_async_copy(half(m, pair, p), piece(m, z, p), r.own_sem.at[p, m]), z
        )

    if extra:

        @pl.when((z + c) % 2 == 1)
        def _():
            for ref in gathered:
                ref[:, pl.ds(base, extra)] = jnp.zeros((features, extra), BF16)

    mate = first_z + 1 - pair
    lowest = (count - first_z) // count
    crossing = [lowest * (count + 1 - q) + (1 - lowest) * ((first_z + q) % count) for q in range(2, count)]
    sources = [*crossing[:1], mate, *crossing[1:]]

    def pump(m, source):
        from_line(m, source).wait_recv()
        relay(m, source).start()

    edge = (z == 0) | (z == count - 1)

    def pump(m, source):
        from_line(m, source).wait_recv()
        relay(m, source).start()

    def start_line(condition, *pieces):
        @pl.when(condition)
        def _():
            for m, target in pieces:
                to_line(m, target).start()

    outward = [[(m, target) for target in crossing] for m in range(3)]
    both_outward = [*outward[0], *outward[1]]
    rest = [*outward[0][1:], (0, mate), (1, mate)]
    early = [(1, mate), *outward[0][1:], outward[1][0]]
    rising = (pair == 0) & ~edge
    falling = (pair == 1) & ~edge
    start_line(edge, outward[0][0])
    start_line(z == 0, (0, mate))
    start_line(z == count - 1, *rest, *outward[1])
    start_line(falling, (0, mate), (1, mate))
    start_line(rising, *both_outward)
    queue = [(0, crossing[0]), (0, mate), (1, mate)]
    queue += [(0, source) for source in crossing[1:]] + [(1, source) for source in crossing]
    marks = [len(queue) * k // 6 for k in range(7)]

    def pumps(first, end):
        for m, source in queue[marks[first] : marks[end]]:
            pump(m, source)

    own_side(0).start()
    for m in range(3):
        own_load(m).start()
    load(r.small_gate, r.gates.at[:, pl.ds(0, width_a)])
    load(r.large_gate, r.gates.at[:, pl.ds(width_a, width_b)])
    load(r.small_out, r.out_rows.at[pl.ds(0, width_a)])
    load(r.large_out, r.out_rows.at[pl.ds(width_a, width_b)])
    me = x * 2 + c
    load(r.residual.at[pl.ds(pl.multiple_of(me * share, share), share)], r.out)

    r.taps[:, pl.ds(0, width_a)] = r.small_taps[...].astype(F32)
    r.taps[:, pl.ds(width_a, width_b)] = r.large_taps[...].astype(F32)
    column = width
    for ref in (r.key_taps, r.query_taps):
        for group in range(ref.shape[1]):
            for k in range(ref.shape[0]):
                r.taps[k : k + 1, pl.ds(column, state_len)] = ref[k, group : group + 1].astype(F32)
            column += state_len
    r.gain[0:1, pl.ds(0, width_a)] = r.small_gain[...].astype(F32)[None]
    r.gain[0:1, pl.ds(width_a, width_b)] = r.large_gain[...].astype(F32)[None]
    for index, ref in enumerate((r.mixer_gain, r.ffn_in_gain, r.ffn_out_gain)):
        r.gains[index : index + 1] = ref[...].astype(F32)[None]
    lanes = lax.broadcasted_iota(jnp.int32, (1, SLOTS), 1)
    decay = jnp.zeros((1, SLOTS), F32)
    for first, heads, ref in ((0, heads_a, r.small_decay), (heads_a, heads_b, r.large_decay)):
        for h in range(heads):
            decay = jnp.where(lanes == first + h, ref[h], decay)

    r.state[...] = jnp.zeros_like(r.state)
    r.total[...] = jnp.zeros_like(r.total)
    causal = lower(BLOCK)
    ones = causal.astype(F32)
    rates = jnp.exp(decay)

    def block_rows(i):
        return pl.ds(pl.multiple_of(i * BLOCK, BLOCK), BLOCK)

    def convolve(i, _):
        here_rows = block_rows(i)
        taps_len = r.taps.shape[0]
        for start in range(0, everything, LANES):
            here = pl.ds(start, LANES)
            now = r.values[here_rows, here]
            extended = jnp.concatenate([r.before[:, here], now], axis=0).astype(F32)
            summed = None
            for k in range(taps_len):
                first = HALO - taps_len + 1 + k
                term = r.taps[k : k + 1, here] * extended[first : first + BLOCK]
                summed = term if summed is None else summed + term
            r.before[:, here] = now[BLOCK - HALO :]
            r.values[here_rows, here] = silu(summed).astype(BF16)
        dt = softplus(r.steps[here_rows])
        cum = exact_dot(ones, -dt * rates)
        tail = cum[BLOCK - 1 : BLOCK]
        scale = dt * jnp.exp(tail - cum)
        kept = jnp.exp(tail)
        r.logs[here_rows] = r.total[...] + cum
        r.total[...] = r.total[...] + tail
        for heads, dim, size, offset, key_at in groups:
            columns_here = pl.ds(offset, size)
            values = r.values[here_rows, columns_here].astype(F32)
            u = (values * spread(scale, heads, dim)).astype(BF16)
            k = r.values[here_rows, pl.ds(key_at, state_len)]
            fresh = lax.dot_general(k, u, (((0,), (0,)), ((), ())), preferred_element_type=F32)
            old = r.state[:, columns_here]
            r.states[i, :, columns_here] = old.astype(BF16)
            r.state[:, columns_here] = old * spread(kept, heads, dim) + fresh
        return 0

    lax.fori_loop(0, blocks, convolve, 0)

    def pack(target, state, log):
        target[:state_len] = state.astype(BF16)
        high = log.astype(BF16)
        low = (log - high.astype(F32)).astype(BF16)
        row = lax.broadcasted_iota(jnp.int32, (TAIL, width), 0)
        both = jnp.where(row == 0, high.astype(F32), jnp.where(row == 1, low.astype(F32), 0.0))
        target[state_len:] = both.astype(BF16)

    def opened(ref):
        tail = ref[state_len:].astype(F32)
        return ref[:state_len].astype(F32), tail[0:1] + tail[1:2]

    pack(
        r.packed,
        r.state[...],
        jnp.concatenate([spread(r.total[...], heads, dim) for heads, dim, *_ in groups], axis=1),
    )
    pair_copy = remote(r.packed, r.beside, r.state_send.at[0], r.state_recv.at[0], side)
    pair_copy.start()
    own_side(1).start()
    own_side(2).start()

    upper = (
        lax.broadcasted_iota(jnp.int32, (BLOCK, BLOCK), 0)
        <= lax.broadcasted_iota(jnp.int32, (BLOCK, BLOCK), 1)
    ).astype(F32)
    same = (
        lax.broadcasted_iota(jnp.int32, (BLOCK, BLOCK), 0)
        == lax.broadcasted_iota(jnp.int32, (BLOCK, BLOCK), 1)
    ).astype(F32)
    lane = lax.broadcasted_iota(jnp.int32, (BLOCK, LANES), 1)

    def inside_block(i, _):
        here_rows = block_rows(i)
        dt = softplus(r.steps[here_rows])
        log = -dt * rates
        cum = exact_dot(ones, log)
        cum_across = exact_across(log, upper)
        dt_across = exact_across(dt, same)
        grown = jnp.exp(cum)
        for heads, dim, size, offset, key_at in groups:
            columns_here = pl.ds(offset, size)
            values = r.values[here_rows, columns_here]
            k = r.values[here_rows, pl.ds(key_at, state_len)]
            q = r.values[here_rows, pl.ds(key_at + 2 * state_len, state_len)]
            scores = lax.dot_general(q, k, (((1,), (1,)), ((), ())), preferred_element_type=F32)
            carried = jnp.dot(q, r.states[i, :, columns_here], preferred_element_type=F32)
            carried = carried * spread(grown, heads, dim)
            inside = []
            span = max(dim, LANES)
            per = span // dim
            for first in range(0, len(heads), per):
                part_values = values[:, first * dim : first * dim + span]
                part = None
                for j in range(per):
                    h = heads[first + j]
                    gap = cum[:, h : h + 1] - cum_across[h : h + 1]
                    decays = jnp.exp(jnp.where(causal, gap, FAR))
                    w = (scores * decays * dt_across[h : h + 1]).astype(BF16)
                    got = jnp.dot(w, part_values, preferred_element_type=F32)
                    part = got if part is None else jnp.where(lane >= j * dim, got, part)
                inside.append(part)
            r.inner[here_rows, columns_here] = jnp.concatenate(inside, axis=1) + carried
        return 0

    lax.fori_loop(0, blocks // 2, inside_block, 0)

    pair_copy.wait_recv()
    mine, mine_log = opened(r.packed)
    theirs, theirs_log = opened(r.beside)
    front = y == 0
    lead = jnp.where(front, mine, theirs)
    lead_log = jnp.where(front, mine_log, theirs_log)
    trail = jnp.where(front, theirs, mine)
    trail_log = jnp.where(front, theirs_log, mine_log)
    r.both[:state_len] = lead * jnp.exp(trail_log) + trail
    r.both[state_len:] = jnp.broadcast_to(lead_log + trail_log, (8, width))
    r.ahead[:state_len] = lead
    r.ahead[state_len:] = jnp.broadcast_to(lead_log, (8, width))
    r.state[...] = jnp.zeros_like(r.state)
    r.before_log[...] = jnp.zeros_like(r.before_log)
    hops = r.passed.shape[0]

    def line_copy(s):
        target = {OUTER: (z + (1 << s)) % count}
        return remote(r.passed.at[s], r.arrived.at[s], r.line_send.at[s], r.line_recv.at[s], target)

    for s in range(hops):

        @pl.when(z + (1 << s) < count)
        def _():
            pack(r.passed.at[s], r.both[:state_len], r.both[state_len : state_len + 1])
            line_copy(s).start()

        if s == 0:
            lax.fori_loop(blocks // 2, blocks, inside_block, 0)
        if s == hops - 1:
            start_line(z == 0, *early)
            start_line(falling, *both_outward)

        @pl.when(z >= 1 << s)
        def _():
            line_copy(s).wait_recv()
            before, before_log = opened(r.arrived.at[s])
            r.state[...] = before * jnp.exp(r.before_log[0:1]) + r.state[...]
            r.before_log[...] = r.before_log[...] + before_log
            r.both[:state_len] = before * jnp.exp(r.both[state_len : state_len + 1]) + r.both[:state_len]
            r.both[state_len:] = r.both[state_len:] + before_log

    @pl.when(y == 1)
    def _():
        r.state[...] = r.state[...] * jnp.exp(r.ahead[state_len : state_len + 1]) + r.ahead[:state_len]

    r.entering[...] = r.state[...].astype(BF16)
    start_line(rising, (0, mate), (1, mate))
    for index in range(4, len(loads)):
        loads[index].wait()

    per_share = share // BLOCK

    def strip(part):
        return pl.ds(pl.multiple_of(part * BLOCK, BLOCK), BLOCK)

    def near_mix(index, part):
        return remote(
            r.mix_core.at[index, strip(part)],
            r.mix_from.at[index, strip(part)],
            r.mix_send.at[index, part],
            r.mix_recv.at[index, part],
            near,
        )

    def across_mix(part):
        return remote(
            r.mix_hop.at[strip(part)],
            r.mix_got.at[strip(part)],
            r.mix_send.at[2, part],
            r.mix_recv.at[2, part],
            across,
        )

    def project(b, _):
        far, other = 1 - b // (2 * per_share), 1 - b % 2
        piece_at = b % (2 * per_share) // 2
        source = flipped(x, far) * 2 + flipped(c, other)
        i = source * per_share + piece_at
        here_rows = block_rows(i)
        grown = jnp.exp(r.logs[here_rows])
        result = None
        for heads, dim, size, offset, key_at in groups:
            columns_here = pl.ds(offset, size)
            q = r.values[here_rows, pl.ds(key_at + 2 * state_len, state_len)]
            carried = jnp.dot(q, r.entering[:, columns_here], preferred_element_type=F32)
            mixed = r.inner[here_rows, columns_here] + carried * spread(grown, heads, dim)
            gated = mixed * silu(r.gates[here_rows, columns_here].astype(F32))
            squares = gated * gated
            span = max(dim, LANES)
            per = span // dim
            normed = []
            for first in range(0, len(heads), per):
                at = first * dim
                part = squares[:, at : at + span]
                means = None
                for j in range(per):
                    if per == 1:
                        means = jnp.sum(part, axis=1, keepdims=True)
                    else:
                        ours = (lane >= j * dim) & (lane < (j + 1) * dim)
                        single = jnp.sum(jnp.where(ours, part, 0.0), axis=1, keepdims=True)
                        means = single if means is None else jnp.where(lane >= j * dim, single, means)
                normed.append(gated[:, at : at + span] * lax.rsqrt(means * (1.0 / dim) + EPS))
            normed = jnp.concatenate(normed, axis=1) * r.gain[:, columns_here]
            product = jnp.dot(normed.astype(BF16), r.out_rows[columns_here], preferred_element_type=F32)
            result = product if result is None else result + product
        part = piece_at
        part_rows = strip(part)

        @pl.when(other == 1)
        def _():
            r.mix_core[far, part_rows] = result.astype(BF16)

        @pl.when(other == 0)
        def _():
            r.mix_local[far, part_rows] = result

        @pl.when(other == 1)
        def _():
            near_mix(far, part).start()

        @pl.when((far == 1) & (other == 0))
        def _():
            near_mix(1, part).wait_recv()
            total = r.mix_local[1, part_rows] + r.mix_from[1, part_rows].astype(F32)
            r.mix_hop[part_rows] = total.astype(BF16)
            across_mix(part).start()

        return 0

    lax.fori_loop(0, blocks, project, 0)
    pumps(0, 2)

    def place(core, d_one, d_two):
        return (flipped(pair, d_one) * 2 + flipped(x, d_two)) * 2 + core

    mine_at = place(c, 0, 0)
    tile = BLOCK // 2

    def norms(i, _):
        here = pl.ds(pl.multiple_of(i * tile, tile), tile)
        mix = r.mix_local[0, here] + r.mix_from[0, here].astype(F32) + r.mix_got[here].astype(F32)
        mixed = r.out[here].astype(F32) + unit_rms(mix) * r.gains[0:1]
        r.mixed[here] = mixed
        r.rows[mine_at, here] = (unit_rms(mixed) * r.gains[1:2]).astype(BF16)
        return 0

    def passing(slot, index, partner, part):
        here = r.rows.at[slot, strip(part)]
        return remote(here, here, r.rows_send.at[index, part], r.rows_recv.at[slot, part], partner)

    def forward(slot, index, partner):
        for part in range(per_share):
            passing(slot, index, partner, part).start()

    def arrive(slot):
        for part in range(per_share):
            passing(slot, 0, near, part).wait_recv()

    for part in range(per_share):
        near_mix(0, part).wait_recv()
        across_mix(part).wait_recv()
        lax.fori_loop(part * BLOCK // tile, (part + 1) * BLOCK // tile, norms, 0)
        for index, partner in enumerate((upright, across, near)):
            passing(mine_at, index, partner, part).start()
    start_line(z == 0, *outward[1][1:])
    to_line(2, mate).start()
    for m, target in outward[2][1:]:
        to_line(m, target).start()
    start_line(first_z > 0, outward[2][0])
    pumps(2, 6)

    def complete(m):
        own_load(m).wait()
        for source in range(count):
            relay(m, source).wait_recv()

    def kept_at(core, j):
        return (1 - core) * j + core * (j % 2 * 2 + j // 2)

    complete(0)

    def masked(hidden):
        column = lax.broadcasted_iota(jnp.int32, hidden.shape, 1)
        held = wide - (z + c) % 2 * extra
        return jnp.where(column < held, hidden, 0.0).astype(BF16)

    def open_gate(slot, at):
        gate = jnp.dot(r.rows[slot], r.gate_all[...], preferred_element_type=F32)
        r.hidden[at] = silu(gate).astype(BF16)

    def gates(j, _):
        d_one, d_two = j % 2, j // 2
        slot = place(c, d_one, d_two)

        @pl.when(j == 1)
        def _():
            for part in range(per_share):
                passing(slot, 0, near, part).wait_recv()
                passing(slot, 3, across, part).start()
            forward(slot, 4, near)

        @pl.when(j > 1)
        def _():
            arrive(slot)
            forward(slot, 3 + j, near)

        open_gate(slot, kept_at(c, j))
        slot = place(1 - c, d_one, d_two)
        arrive(slot)
        open_gate(slot, 4 + kept_at(1 - c, j))
        return 0

    lax.fori_loop(0, 3, gates, 0)
    complete(1)

    def expand(j, _):
        for core, first in ((c, 0), (1 - c, 4)):
            at = first + kept_at(core, j)
            up = jnp.dot(r.rows[place(core, j % 2, j // 2)], r.up_all[...], preferred_element_type=F32)
            r.hidden[at] = masked(r.hidden[at].astype(F32) * up)
        return 0

    lax.fori_loop(0, 3, expand, 0)
    start_line(first_z == 0, outward[2][0])
    pump(2, mate)
    for part in range(per_share):
        for core, at in ((c, 3), (1 - c, 7)):
            slot = place(core, 1, 1)
            passing(slot, 0, near, part).wait_recv()
            if at == 3:
                passing(slot, 6, near, part).start()
            values = r.rows[slot, strip(part)]
            gate = jnp.dot(values, r.gate_all[...], preferred_element_type=F32)
            up = jnp.dot(values, r.up_all[...], preferred_element_type=F32)
            r.hidden[at, strip(part)] = masked(silu(gate) * up)

    chunk = r.got_one.shape[-1]
    per_chunk = chunk // rows
    chunks = features // chunk
    first_chunk = 2 * first_z * rows // chunk

    def chunk_at(k):
        return (first_chunk + k) % chunks

    def pump_chunk(k):
        for index in range(per_chunk):
            block = chunk_at(k) * per_chunk + index

            @pl.when((block % 2 == y) & (block // 2 // 2 != z // 2))
            def _():
                pump(2, block // 2)

    def near_copy(k):
        return remote(
            r.to_core.at[k % RING], r.from_core.at[k], r.core_send.at[k % RING], r.core_recv.at[k], near
        )

    def two_copy(k):
        return remote(r.hop_two.at[k % RING], r.got_two.at[k], r.two_send.at[k % RING], r.two_recv.at[k], two)

    def one_copy(k):
        return remote(r.hop_one.at[k % RING], r.got_one.at[k], r.one_send.at[k % RING], r.one_recv.at[k], one)

    def local_at(k, j):
        slot = k % RING
        start = pl.multiple_of((slot % 2 * 4 + j) * chunk, LANES)
        return slot // 2, slice(None), pl.ds(start, chunk)

    own_load(2).wait()
    for k in range(AHEAD):
        pump_chunk(k)

    def reduce_step(k, _):
        @pl.when((k >= 1) & (k < chunks + 1))
        def _():
            p = k - 1
            near_copy(p).wait_recv()

            @pl.when(p >= RING)
            def _():
                two_copy(p).wait_send()

            for index, j in enumerate((3, 2)):
                total = r.mix_local[local_at(p, j)] + r.from_core[p, j].astype(F32)
                r.hop_two[p % RING, index] = total.astype(BF16)
            two_copy(p).start()
            for j in range(2):
                r.mix_local[local_at(p, j)] = r.mix_local[local_at(p, j)] + r.from_core[p, j].astype(F32)

        @pl.when(k < chunks)
        def _():
            for index in range(per_chunk):
                block = chunk_at(k) * per_chunk + index

                @pl.when(block % 2 != y)
                def _():
                    relay(2, block // 2).wait_recv()

            @pl.when(k >= RING)
            def _():
                near_copy(k).wait_send()

            at = pl.ds(pl.multiple_of(chunk_at(k) * chunk, chunk), chunk)
            weights = r.down_all[at]
            for j in range(4):
                r.to_core[k % RING, j] = lax.dot_general(
                    r.hidden[4 + j], weights, (((1,), (1,)), ((), ())), preferred_element_type=F32
                ).astype(BF16)
            near_copy(k).start()
            for j in range(4):
                r.mix_local[local_at(k, j)] = lax.dot_general(
                    r.hidden[j], weights, (((1,), (1,)), ((), ())), preferred_element_type=F32
                )

        @pl.when((k >= 2) & (k < chunks + 2))
        def _():
            p = k - 2
            two_copy(p).wait_recv()

            @pl.when(p >= RING)
            def _():
                one_copy(p).wait_send()

            total = r.mix_local[local_at(p, 1)] + r.got_two[p, 0].astype(F32)
            r.hop_one[p % RING] = total.astype(BF16)
            one_copy(p).start()

        @pl.when(k >= 3)
        def _():
            p = k - 3
            one_copy(p).wait_recv()
            total = r.mix_local[local_at(p, 0)] + r.got_two[p, 1].astype(F32) + r.got_one[p].astype(F32)
            r.ffn[:, pl.ds(pl.multiple_of(chunk_at(p) * chunk, chunk), chunk)] = total

        @pl.when(k < chunks - AHEAD)
        def _():
            pump_chunk(k + AHEAD)

        return 0

    lax.fori_loop(0, chunks + 3, reduce_step, 0)

    def finish(i, _):
        here = pl.ds(pl.multiple_of(i * tile, tile), tile)
        r.out[here] = (r.mixed[here] + 0.5 * unit_rms(r.ffn[here]) * r.gains[2:3]).astype(BF16)
        return 0

    lax.fori_loop(0, share // tile, finish, 0)

    @pl.when(~last)
    def _():
        for index in range(4):
            halo_copy(index, side).wait_send()

    pair_copy.wait_send()

    for s in range(hops):

        @pl.when(z + (1 << s) < count)
        def _():
            line_copy(s).wait_send()

    for m in range(3):
        for target in sources:
            to_line(m, target).wait_send()
        for source in range(count):
            relay(m, source).wait_send()
    for part in range(per_share):
        near_mix(0, part).wait_send()
        near_mix(1, part).wait_send()
        across_mix(part).wait_send()
        for index in range(7):
            passing(mine_at, index, near, part).wait_send()
    for slot in range(min(RING, chunks)):
        near_copy(slot).wait_send()
        two_copy(slot).wait_send()
        one_copy(slot).wait_send()


def layer(
    residual,
    small_heads,
    large_heads,
    state_keys,
    state_queries,
    small_gate,
    large_gate,
    small_step,
    large_step,
    small_taps,
    large_taps,
    key_taps,
    query_taps,
    small_decay,
    large_decay,
    small_gain,
    large_gain,
    small_out,
    large_out,
    mixer_gain,
    ffn_in_gain,
    gate_proj,
    up_proj,
    down_proj,
    ffn_out_gain,
):
    length, features = residual.shape
    state_len = state_keys.shape[-1]
    key_rows = state_keys.reshape(length, -1)
    query_rows = state_queries.reshape(length, -1)
    heads_a = small_step.shape[1]
    heads_b = large_step.shape[1]
    heads = heads_a + heads_b
    width_a = small_heads.shape[1]
    width_b = large_heads.shape[1]
    width = width_a + width_b
    everything = width + key_rows.shape[1] + query_rows.shape[1]
    sizes = ((heads_a, width_a // heads_a), (heads_b, width_b // heads_b), state_len)
    steps = jnp.pad(
        jnp.concatenate([small_step, large_step], axis=1), ((0, 0), (0, SLOTS - heads))
    )
    taps_len = small_taps.shape[0]
    share = length // lax.axis_size(HEADS)
    rows, columns = down_proj.shape
    count = lax.axis_size(OUTER)
    wide = half_width(columns)
    chunk = max(rows, CHUNK)
    chunks = features // chunk
    blocks = length // BLOCK
    vmem = pl.BlockSpec(memory_space=pltpu.VMEM)
    hbm = pl.BlockSpec(memory_space=pl.ANY)
    smem = pl.BlockSpec(memory_space=pltpu.SMEM)
    dma = pltpu.SemaphoreType.DMA
    operands = {
        "small": (small_heads, hbm),
        "large": (large_heads, hbm),
        "keys": (key_rows, hbm),
        "queries": (query_rows, hbm),
        "small_gate": (small_gate, hbm),
        "large_gate": (large_gate, hbm),
        "small_out": (small_out, hbm),
        "large_out": (large_out, hbm),
        "residual": (residual, hbm),
        "gate_proj": (gate_proj, hbm),
        "up_proj": (up_proj, hbm),
        "down_proj": (down_proj, hbm),
        "steps": (steps, vmem),
        "small_decay": (small_decay, smem),
        "large_decay": (large_decay, smem),
        "small_taps": (small_taps, vmem),
        "large_taps": (large_taps, vmem),
        "key_taps": (key_taps, vmem),
        "query_taps": (query_taps, vmem),
        "small_gain": (small_gain, vmem),
        "large_gain": (large_gain, vmem),
        "mixer_gain": (mixer_gain, vmem),
        "ffn_in_gain": (ffn_in_gain, vmem),
        "ffn_out_gain": (ffn_out_gain, vmem),
    }
    packed = (state_len + TAIL, width)
    opened = (state_len + 8, width)
    hops = max(1, (count - 1).bit_length())
    scratch = {
        "values": pltpu.VMEM((length, everything), BF16),
        "gates": pltpu.VMEM((length, width), BF16),
        "out_rows": pltpu.VMEM((width, features), BF16),
        "gate_all": pltpu.VMEM((features, wide), BF16),
        "up_all": pltpu.VMEM((features, wide), BF16),
        "down_all": pltpu.VMEM((features, wide), BF16),
        "taps": pltpu.VMEM((taps_len, everything), F32),
        "gain": pltpu.VMEM((1, width), F32),
        "gains": pltpu.VMEM((3, features), F32),
        "halo": pltpu.VMEM((HALO, everything), BF16),
        "before": pltpu.VMEM((HALO, everything), BF16),
        "state": pltpu.VMEM((state_len, width), F32),
        "states": pltpu.VMEM((blocks, state_len, width), BF16),
        "total": pltpu.VMEM((1, SLOTS), F32),
        "logs": pltpu.VMEM((length, SLOTS), F32),
        "inner": pltpu.VMEM((length, width), F32),
        "packed": pltpu.VMEM(packed, BF16),
        "beside": pltpu.VMEM(packed, BF16),
        "passed": pltpu.VMEM((hops, *packed), BF16),
        "arrived": pltpu.VMEM((hops, *packed), BF16),
        "before_log": pltpu.VMEM((8, width), F32),
        "both": pltpu.VMEM(opened, F32),
        "ahead": pltpu.VMEM(opened, F32),
        "entering": pltpu.VMEM((state_len, width), BF16),
        "mix_core": pltpu.VMEM((2, share, features), BF16),
        "mix_from": pltpu.VMEM((2, share, features), BF16),
        "mix_local": pltpu.VMEM((2, share, features), F32),
        "mix_hop": pltpu.VMEM((share, features), BF16),
        "mix_got": pltpu.VMEM((share, features), BF16),
        "mixed": pltpu.VMEM((share, features), F32),
        "rows": pltpu.VMEM((8, share, features), BF16),
        "hidden": pltpu.VMEM((8, share, wide), BF16),
        "to_core": pltpu.VMEM((RING, 4, share, chunk), BF16),
        "from_core": pltpu.VMEM((chunks, 4, share, chunk), BF16),
        "hop_two": pltpu.VMEM((RING, 2, share, chunk), BF16),
        "got_two": pltpu.VMEM((chunks, 2, share, chunk), BF16),
        "hop_one": pltpu.VMEM((RING, share, chunk), BF16),
        "got_one": pltpu.VMEM((chunks, share, chunk), BF16),
        "ffn": pltpu.VMEM((share, features), F32),
        "halo_send": dma((4,)),
        "halo_recv": dma((4,)),
        "load_sem": dma((9,)),
        "own_sem": dma((2, 3)),
        "send": dma((2, 3, count)),
        "recv": dma((2, 3, count)),
        "side_send": dma((2, 3, count)),
        "side_recv": dma((2, 3, count)),
        "state_send": dma((1,)),
        "state_recv": dma((1,)),
        "line_send": dma((hops,)),
        "line_recv": dma((hops,)),
        "mix_send": dma((3, share // BLOCK)),
        "mix_recv": dma((3, share // BLOCK)),
        "rows_send": dma((7, share // BLOCK)),
        "rows_recv": dma((8, share // BLOCK)),
        "core_send": dma((RING,)),
        "core_recv": dma((chunks,)),
        "two_send": dma((RING,)),
        "two_recv": dma((chunks,)),
        "one_send": dma((RING,)),
        "one_recv": dma((chunks,)),
    }
    names = (*operands, "out", *scratch)
    return pl.pallas_call(
        functools.partial(layer_kernel, names, sizes, columns - wide),
        in_specs=[spec for _, spec in operands.values()],
        out_specs=vmem,
        out_shape=jax.ShapeDtypeStruct((share, features), BF16),
        scratch_shapes=list(scratch.values()),
        compiler_params=pltpu.CompilerParams(
            collective_id=0, has_side_effects=True, vmem_limit_bytes=VMEM_BYTES
        ),
        cost_estimate=pl.CostEstimate(
            flops=40_000_000_000, bytes_accessed=share * features, transcendentals=0
        ),
        name="layer",
    )(*[array for array, _ in operands.values()])


def solution(mesh):
    placed = (
        P(SEQ, None),
        P(SEQ, HEADS),
        P(SEQ, HEADS),
        P(SEQ, HEADS, None),
        P(SEQ, HEADS, None),
        P(SEQ, HEADS),
        P(SEQ, HEADS),
        P(SEQ, HEADS),
        P(SEQ, HEADS),
        P(None, HEADS),
        P(None, HEADS),
        P(None, HEADS, None),
        P(None, HEADS, None),
        P(HEADS),
        P(HEADS),
        P(HEADS),
        P(HEADS),
        P(HEADS, None),
        P(HEADS, None),
        P(),
        P(),
        P(SEQ, HEADS),
        P(SEQ, HEADS),
        P(SEQ, HEADS),
        P(),
    )
    outer, heads = mesh.shape["sp"] // 2, mesh.shape["tp"] // 2
    cut = jax.sharding.Mesh(mesh.devices.reshape(outer, 2, heads, 2), (OUTER, INNER, CHIP, CORE))
    return jax.shard_map(
        layer, mesh=cut, in_specs=placed, out_specs=P((*SEQ, *HEADS), None), check_vma=False
    )
```
